32 devices in a mesh: sp: 16 (over z, y, x), tp: 2 (over core).
Axes of the slice: x: 2, y: 2, z: 4, core: 2. Of those that a mesh axis runs over, the one named last changes fastest.
Arguments:
- moe_input: bfloat16 [4096, 2048], P('sp'), may hold values from -6 to 6
- cotangent: bfloat16 [4096, 2048], P('sp'), may hold values from -6 to 6
- expert_ids: int32 [4096, 2], P('sp'), may hold values from 0 to 15, all different within a row; in each aligned block of 256 rows (0 to 255, 256 to 511, ...) at most 64 rows name the same one
- route_weight: float32 [4096, 2], P('sp'), may hold values from 0.05 to 0.6
- gate_proj: bfloat16 [16, 2048, 1024], P('sp', None, 'tp'), may hold values from -0.125 to 0.125
- up_proj: bfloat16 [16, 2048, 1024], P('sp', None, 'tp'), may hold values from -0.125 to 0.125
- down_proj: bfloat16 [16, 1024, 2048], P('sp', 'tp'), may hold values from -0.1875 to 0.1875
- out_weight: bfloat16 [2048, 2048], P(None, 'tp'), may hold values from -0.125 to 0.125
- recur_input: bfloat16 [4096, 2048], P('sp', 'tp'), may hold values from -6 to 6
- gate_input: bfloat16 [4096, 2048], P('sp', 'tp'), may hold values from -6 to 6
- states: float32 [4096, 2048], P('sp', 'tp'), may hold values from -6 to 6
- conv_taps: bfloat16 [4, 2048], P(None, 'tp'), may hold values from -3 to 3
- decay_gate_w: bfloat16 [16, 128, 128], P('tp'), may hold values from -0.5 to 0.5
- input_gate_w: bfloat16 [16, 128, 128], P('tp'), may hold values from -0.5 to 0.5
- decay_rate: float32 [2048], P('tp'), may hold values from 7.3242187e-06 to 0.008
- decay_extra: float32 [4096, 2048], P('sp', 'tp'), may hold values from -0.77 to 0
Outputs:
- gate_proj_grad: bfloat16 [16, 2048, 1024], P('sp', None, 'tp')
- up_proj_grad: bfloat16 [16, 2048, 1024], P('sp', None, 'tp')
- down_proj_grad: bfloat16 [16, 1024, 2048], P('sp', 'tp')
- out_weight_grad: float32 [2048, 2048], P('sp', 'tp')
- input_grad: bfloat16 [4096, 2048], P('sp')
- recur_grad: bfloat16 [4096, 2048], P('sp', 'tp')
- gate_grad: bfloat16 [4096, 2048], P('sp', 'tp')
The draws below stay inside these ranges and needn't reach their ends.
Inputs may be any that keep to these rules, and one draw needn't show every extreme that they name: `expert_ids`: within each aligned block of 256 tokens a token names 2 different experts, and no expert is named more than 64 times.
All inputs are finite; a program needn't handle non-finite values.
Results may differ from the reference program's by a relative error of at most 0.012.
Values may be sent and summed in bfloat16 or wider, within the bound.
No kernel may reach another device: no remote copies, remote signals or barrier semaphores. Data moves between devices by JAX's collectives and lax.ppermute only.
A program may use at most 128 MiB of HBM per device.

```python
import math
import jax
import jax.numpy as jnp
import numpy as np
from jax import lax

D = 2048
FF = 1024
RECURRENCE_WIDTH = 2048
LRU_BLOCKS = 16
TOPK = 2
TOK_DEV = 256
BLK = 128
SEQUENCE_TOKENS = 4096
EXPERTS = 16
CAP = 64
N_SP = 16
N_TP = 2


def decay_parts(key):
    base_key = jax.random.fold_in(key, 4242)
    multiple_count = jax.random.split(base_key, 6)
    fast_share = 0.5
    fast_mask = jax.random.uniform(multiple_count[0], (RECURRENCE_WIDTH,), jnp.float32) < fast_share
    slow_rate = jnp.exp(jax.random.uniform(multiple_count[1], (RECURRENCE_WIDTH,), jnp.float32, math.log(0.03 / SEQUENCE_TOKENS), math.log(0.15 / SEQUENCE_TOKENS)))
    fast_rate = jnp.exp(jax.random.uniform(multiple_count[2], (RECURRENCE_WIDTH,), jnp.float32, math.log(0.0025), math.log(0.008)))
    rate_value = jnp.where(fast_mask, fast_rate, slow_rate)
    block_count = SEQUENCE_TOKENS // TOK_DEV
    factor = jax.random.uniform(multiple_count[3], (block_count, RECURRENCE_WIDTH), jnp.float32, 0.0, 2.0)
    gentle_component = jnp.repeat(-4.0 * rate_value[None, :] * factor, TOK_DEV, axis=0)
    spike_indicator = jax.random.uniform(multiple_count[4], (SEQUENCE_TOKENS, RECURRENCE_WIDTH), jnp.float32) < 3.0 / SEQUENCE_TOKENS
    spike_magnitude = jax.random.uniform(multiple_count[5], (SEQUENCE_TOKENS, RECURRENCE_WIDTH), jnp.float32, 0.22, 0.7)
    additional_value = gentle_component - jnp.where(spike_indicator, spike_magnitude, 0.0)
    return (rate_value, additional_value)


def draw_decay_rate(key, part):
    return decay_parts(key)[0]


def draw_decay_extra(key, part):
    return decay_parts(key)[1]


def with_spikes(drawn, own_key, source, target, blocks, factor):
    def block_of(axis_at):
        return (jnp.arange(drawn.shape[axis_at]) // (drawn.shape[axis_at] // blocks)).reshape((-1,) + (1,) * (drawn.ndim - 1 - axis_at))

    near = jax.random.permutation(own_key, blocks)[block_of(target)]
    second = (block_of(target) + blocks // 2) % blocks
    return jnp.where((block_of(source) == near) | (block_of(source) == second), factor * drawn, drawn)


def levels(key, shape, shards, low, high):
    def one(axis_at, shards_of):
        draws = jax.random.uniform(jax.random.fold_in(jax.random.fold_in(key, 6), axis_at), (shards_of,), jnp.float32, low / len(shards), high / len(shards))
        return jnp.repeat(jnp.exp(draws), shape[axis_at] // shards_of).reshape((-1,) + (1,) * (len(shape) - axis_at - 1))

    loudness = one(*shards[0])
    for cut in shards[1:]:
        loudness = loudness * one(*cut)
    return loudness


def shared_out(own_key, own, number, rows, count, top, limit, lean):
    order = jax.random.permutation(own_key, count)
    heavy_load, ordinary = shares(count, rows * top, limit, lean, True), shares(count, rows * top, limit, lean, False)
    places = jnp.arange(count)

    def named(sizes, turn):
        used = int((sizes > 0).sum())
        fixed = max(1, used // 4)
        passed = fixed + (places - fixed + turn * (used - fixed)) % max(1, count - fixed)
        return jnp.zeros((count,), jnp.int32).at[order[jnp.where(places < fixed, places, passed)]].set(jnp.asarray(sizes, jnp.int32))

    sizes = jnp.where(number % 4 == 0, named(heavy_load, number // 4), named(ordinary, number - number // 4 - 1))
    mixed = jax.random.permutation(jax.random.fold_in(own, 3), count)
    donor, taker = mixed[0:count // 2 * 2:2], mixed[1:count // 2 * 2:2]
    margin = jnp.minimum(sizes[donor] - 1, limit - sizes[taker]) // 2
    margin = jnp.where((donor == order[0]) | (taker == order[0]) | (sizes[taker] == 0), 0, jnp.maximum(margin, 0))
    passed = jax.random.randint(jax.random.fold_in(own, 4), (count // 2,), 0, 1 << 20) % (margin + 1)
    sizes = sizes.at[donor].add(-passed).at[taker].add(passed)
    items = jnp.searchsorted(jnp.cumsum(sizes), jnp.arange(rows * top), side="right").astype(jnp.int32)
    grid = items.reshape(top, rows).T
    grid = grid[jax.random.permutation(jax.random.fold_in(own, 1), rows)]
    turn = jax.random.randint(jax.random.fold_in(own, 2), (rows, 1), 0, top)
    return jnp.take_along_axis(grid, (jnp.arange(top)[None, :] + turn) % top, axis=1)


def shares(amount, total, limit, lean, full):
    loads = [(1 << 20) // math.isqrt(rank ** lean) + 1 for rank in range(1, amount + 1)]
    largest = limit if full else min(limit, max(-(-total // amount), total * loads[0] // sum(loads)))
    least = 1 if total - largest >= amount - 1 else 0
    holding, surplus = [largest] + [least] * (amount - 1), total - largest - least * (amount - 1)
    while surplus > 0:
        free = [i for i in range(1, amount) if holding[i] < largest] or [i for i in range(1, amount) if holding[i] < limit]
        whole, left = sum([loads[i] for i in free]), surplus
        for i in free:
            extra = min(limit - holding[i], max(1, left * loads[i] // whole), surplus)
            holding[i] = holding[i] + extra
            surplus = surplus - extra
    return np.array(holding)


def bell_draw(key, dims, width, reach, cuts=(), kind=jnp.bfloat16):
    entries = width * jax.random.normal(key, dims, jnp.float32)
    if cuts:
        entries = entries * levels(key, dims, cuts, -0.22, 0.18)
    return jnp.clip(entries, -reach, reach).astype(kind)


def heavy_noise(own_key, shape, deviation, most, pieces, heavy, kind=jnp.bfloat16):
    values = deviation * jax.random.normal(own_key, shape, jnp.float32)
    if pieces:
        values = values * levels(own_key, shape, pieces, -0.22, 0.18)
    return jnp.clip(with_spikes(values, jax.random.fold_in(own_key, 3), *heavy), -most, most).astype(kind)


def setup_inputs(seed: int = 0) -> dict:
    keys = jax.random.split(jax.random.key(seed), 17)
    moe_input = bell_draw(keys[0], (SEQUENCE_TOKENS, D), 1.0, 6.0, ((0, 16),))
    cotangent = heavy_noise(keys[1], (SEQUENCE_TOKENS, D), 1.0, 6.0, ((0, 16),), (0, 1, 16, 2.0))
    expert_ids_keys = jax.random.split(jax.random.fold_in(keys[2], 1), SEQUENCE_TOKENS // TOK_DEV)
    expert_ids_turns = jax.random.permutation(jax.random.fold_in(keys[2], 3), SEQUENCE_TOKENS // TOK_DEV)
    expert_ids = jax.vmap(lambda own, number: shared_out(jax.random.fold_in(keys[2], 2), own, number, TOK_DEV, EXPERTS, TOPK, CAP, 1))(expert_ids_keys, expert_ids_turns).reshape((SEQUENCE_TOKENS, TOPK))
    route_weight = jnp.clip(0.05 + 0.55 * jax.random.uniform(keys[3], (SEQUENCE_TOKENS, TOPK), jnp.float32) ** levels(keys[3], (SEQUENCE_TOKENS, TOPK), ((0, 16),), -0.2, 0.2), 0.05, 0.6)
    gate_proj = bell_draw(keys[4], (EXPERTS, D, FF), D ** -0.5, 0.125, ((0, 16), (2, 2)))
    up_proj = bell_draw(keys[5], (EXPERTS, D, FF), D ** -0.5, 0.125, ((0, 16), (2, 2)))
    down_proj = bell_draw(keys[6], (EXPERTS, FF, D), FF ** -0.5, 0.1875, ((0, 16), (1, 2)))
    out_weight = bell_draw(keys[7], (D, RECURRENCE_WIDTH), RECURRENCE_WIDTH ** -0.5, 0.125, ((1, 2),))
    recur_input = bell_draw(keys[8], (SEQUENCE_TOKENS, RECURRENCE_WIDTH), 1.0, 6.0, ((0, 16), (1, 2)))
    gate_input = bell_draw(keys[9], (SEQUENCE_TOKENS, RECURRENCE_WIDTH), 1.0, 6.0, ((0, 16), (1, 2)))
    states = bell_draw(keys[10], (SEQUENCE_TOKENS, RECURRENCE_WIDTH), 1.0, 6.0, ((0, 16), (1, 2)), jnp.float32)
    conv_taps = bell_draw(keys[11], (4, RECURRENCE_WIDTH), 4 ** -0.5, 3.0, ((1, 2),))
    decay_gate_w = bell_draw(keys[12], (LRU_BLOCKS, BLK, BLK), BLK ** -0.5, 0.5, ((0, 2),))
    input_gate_w = bell_draw(keys[13], (LRU_BLOCKS, BLK, BLK), BLK ** -0.5, 0.5, ((0, 2),))
    decay_rate = draw_decay_rate(jax.random.fold_in(keys[16], 71), 0)
    decay_extra = draw_decay_extra(jax.random.fold_in(keys[16], 71), 0)
    return dict(moe_input=moe_input, cotangent=cotangent, expert_ids=expert_ids, route_weight=route_weight, gate_proj=gate_proj, up_proj=up_proj, down_proj=down_proj, out_weight=out_weight, recur_input=recur_input, gate_input=gate_input, states=states, conv_taps=conv_taps, decay_gate_w=decay_gate_w, input_gate_w=input_gate_w, decay_rate=decay_rate, decay_extra=decay_extra)


decay_scale = 8.0

def pair_combine(earlier, later):
    return (earlier[0] * later[0], later[0] * earlier[1] + later[1])

def rounded(value):
    return lax.optimization_barrier(value.astype(jnp.bfloat16)).astype(jnp.float32)

def slot_layout(expert_ids):
    source_ids = expert_ids.reshape(N_SP, TOK_DEV * TOPK)
    onehot = (source_ids[:, :, None] == jnp.arange(EXPERTS, dtype=jnp.int32)[None, None, :]).astype(jnp.int32)
    slot_rank = lax.optimization_barrier(jnp.sum((jnp.cumsum(onehot, axis=1) - onehot) * onehot, axis=2))
    sources = jnp.arange(N_SP, dtype=jnp.int32)[:, None]
    target = ((source_ids * N_SP + sources) * CAP + slot_rank).reshape(-1).astype(jnp.int32)
    source_table = jnp.full((EXPERTS * N_SP * CAP,), SEQUENCE_TOKENS * TOPK, jnp.int32)
    source_table = source_table.at[target].set(jnp.arange(SEQUENCE_TOKENS * TOPK, dtype=jnp.int32))
    return (source_table.reshape(EXPERTS, N_SP * CAP), target)

def reference(moe_input, cotangent, expert_ids, route_weight, gate_proj, up_proj, down_proj, out_weight, recur_input, gate_input, states, conv_taps, decay_gate_w, input_gate_w, decay_rate, decay_extra):
    cot_float = cotangent.astype(jnp.float32)
    scaled = (route_weight[:, :, None] * cot_float[:, None, :]).astype(jnp.bfloat16).reshape(SEQUENCE_TOKENS * TOPK, D)
    token_rows = jnp.repeat(moe_input, TOPK, axis=0)
    zero_row = jnp.zeros((1, D), jnp.bfloat16)
    padded_rows = jnp.concatenate([token_rows, zero_row], axis=0)
    padded_cot = jnp.concatenate([scaled, zero_row], axis=0)
    source_table, target = slot_layout(expert_ids)

    def one_expert(inputs):
        slot_index, weight_gate, weight_up, weight_down = inputs
        rows_float = padded_rows[slot_index].astype(jnp.float32)
        cot_rows = padded_cot[slot_index].astype(jnp.float32)
        gate_float = weight_gate.astype(jnp.float32)
        up_float = weight_up.astype(jnp.float32)
        down_float = weight_down.astype(jnp.float32)
        gate_pre = jnp.dot(rows_float, gate_float)
        up_pre = jnp.dot(rows_float, up_float)
        sigmoid_gate = jax.nn.sigmoid(gate_pre)
        silu_gate = gate_pre * sigmoid_gate
        hidden = rounded(silu_gate * up_pre)
        down_grad = jnp.dot(hidden.T, cot_rows)
        hidden_grad = jnp.dot(cot_rows, down_float.T)
        gate_pre_grad = rounded(hidden_grad * up_pre * sigmoid_gate * (1.0 + gate_pre * (1.0 - sigmoid_gate)))
        up_pre_grad = rounded(hidden_grad * silu_gate)
        gate_weight_grad = jnp.dot(rows_float.T, gate_pre_grad)
        up_weight_grad = jnp.dot(rows_float.T, up_pre_grad)
        share_size = FF // N_TP
        summed = jnp.zeros((N_SP * CAP, D), jnp.float32)
        for part_index in range(N_TP):
            lower = part_index * share_size
            upper = lower + share_size
            piece_grad = jnp.dot(gate_pre_grad[:, lower:upper], gate_float[:, lower:upper].T) + jnp.dot(up_pre_grad[:, lower:upper], up_float[:, lower:upper].T)
            summed = summed + rounded(piece_grad)
        return (gate_weight_grad.astype(jnp.bfloat16), up_weight_grad.astype(jnp.bfloat16), down_grad.astype(jnp.bfloat16), summed.astype(jnp.bfloat16))
    gate_proj_grad, up_proj_grad, down_proj_grad, slot_grad = lax.map(one_expert, (source_table, gate_proj, up_proj, down_proj))
    gathered = slot_grad.reshape(EXPERTS * N_SP * CAP, D)[target].astype(jnp.float32)
    gathered = gathered.reshape(SEQUENCE_TOKENS, TOPK, D)
    moe_grad = gathered[:, 0]
    for choice_index in range(1, TOPK):
        moe_grad = moe_grad + gathered[:, choice_index]
    input_grad = (moe_grad + cot_float).astype(jnp.bfloat16)
    grad_float = input_grad.astype(jnp.float32)
    gate_float_in = gate_input.astype(jnp.float32)
    gelu_value, gelu_back = jax.vjp(jax.nn.gelu, gate_float_in)
    mixer_out = (states * gelu_value).astype(jnp.bfloat16).astype(jnp.float32)
    out_weight_grad = jnp.dot(grad_float.T, mixer_out)
    mixer_grad = jnp.dot(grad_float, out_weight.astype(jnp.float32))
    gate_grad = gelu_back(mixer_grad * states)[0].astype(jnp.bfloat16)
    state_grad = mixer_grad * gelu_value
    taps = conv_taps.astype(jnp.float32)
    padded_in = jnp.pad(recur_input.astype(jnp.float32), ((3, 0), (0, 0)))
    conv = taps[0] * padded_in[0:SEQUENCE_TOKENS]
    for tap_index in range(1, 4):
        conv = conv + taps[tap_index] * padded_in[tap_index:tap_index + SEQUENCE_TOKENS]
    conv_blocks = rounded(conv).reshape(SEQUENCE_TOKENS, LRU_BLOCKS, BLK)
    decay_w = decay_gate_w.astype(jnp.float32)
    input_w = input_gate_w.astype(jnp.float32)
    decay_pre = jnp.einsum('tbi,bij->tbj', conv_blocks, decay_w).reshape(SEQUENCE_TOKENS, RECURRENCE_WIDTH)
    input_pre = jnp.einsum('tbi,bij->tbj', conv_blocks, input_w).reshape(SEQUENCE_TOKENS, RECURRENCE_WIDTH)
    recur_gate = jax.nn.sigmoid(decay_pre)
    input_gate = jax.nn.sigmoid(input_pre)
    positions = jnp.arange(SEQUENCE_TOKENS, dtype=jnp.int32)
    first_row = (positions == 0)[:, None]
    log_decay = -decay_scale * recur_gate * decay_rate[None, :] + decay_extra
    decay_value = jnp.exp(log_decay)
    mult = jnp.where(first_row, 1.0, jnp.sqrt(-jnp.expm1(2.0 * log_decay)))
    prev_states = jnp.concatenate([jnp.zeros((1, RECURRENCE_WIDTH), jnp.float32), states[:-1]], axis=0)
    next_decay = jnp.concatenate([decay_value[1:], jnp.zeros((1, RECURRENCE_WIDTH), jnp.float32)], axis=0)
    cumul_flip, values_flip = lax.associative_scan(pair_combine, (next_decay[::-1], state_grad[::-1]), axis=0)
    carried_grad = values_flip[::-1]
    log_grad = carried_grad * prev_states * decay_value - jnp.where(first_row, 0.0, carried_grad * input_gate * conv * decay_value * decay_value / mult)
    decay_pre_grad = rounded(log_grad * (-decay_scale * decay_rate[None, :]) * recur_gate * (1.0 - recur_gate))
    input_pre_grad = rounded(carried_grad * mult * conv * input_gate * (1.0 - input_gate))
    conv_grad = carried_grad * mult * input_gate + jnp.einsum('tbj,bij->tbi', decay_pre_grad.reshape(SEQUENCE_TOKENS, LRU_BLOCKS, BLK), decay_w).reshape(SEQUENCE_TOKENS, RECURRENCE_WIDTH) + jnp.einsum('tbj,bij->tbi', input_pre_grad.reshape(SEQUENCE_TOKENS, LRU_BLOCKS, BLK), input_w).reshape(SEQUENCE_TOKENS, RECURRENCE_WIDTH)
    padded_grad = jnp.pad(conv_grad, ((0, 3), (0, 0)))
    recur_float = taps[0] * padded_grad[3:3 + SEQUENCE_TOKENS]
    for tap_index in range(1, 4):
        recur_float = recur_float + taps[tap_index] * padded_grad[3 - tap_index:3 - tap_index + SEQUENCE_TOKENS]
    recur_grad = recur_float.astype(jnp.bfloat16)
    return (gate_proj_grad, up_proj_grad, down_proj_grad, out_weight_grad, input_grad, recur_grad, gate_grad)
```

```python
import functools

import jax
import jax.numpy as jnp
from jax import lax
from jax.experimental import pallas as pl
from jax.experimental.pallas import tpu as pltpu
from jax.sharding import PartitionSpec as P

decay_scale = 8.0
f32 = jnp.float32
bf16 = jnp.bfloat16


def dot(left, right, contract):
    return lax.dot_general(left, right, (contract, ((), ())), preferred_element_type=f32)


def rows_of(left, right):
    return dot(left, right, ((0,), (0,)))


def cols_of(left, right):
    return dot(left, right, ((1,), (1,)))


def times(left, right):
    return dot(left, right, ((1,), (0,)))


def shifted(value, axis, steps):
    count = lax.axis_size(axis)
    pairs = [(s, s + steps) for s in range(max(0, -steps), min(count, count - steps))]
    return lax.ppermute(value, axis, pairs)


def swapped(value, axis, mask):
    count = lax.axis_size(axis)
    return lax.ppermute(value, axis, [(s, s ^ mask) for s in range(count)])


def back_scan(decays, values):
    rows = values.shape[0]
    inner = lax.broadcasted_iota(jnp.int32, values.shape, 0) % 8
    step = 1
    while step < rows:
        if step < 8:
            keep = inner < 8 - step
            later_a = jnp.where(keep, pltpu.roll(decays, rows - step, 0), 1.0)
            later_b = jnp.where(keep, pltpu.roll(values, rows - step, 0), 0.0)
            values = values + decays * later_b
            decays = decays * later_a
            step *= 2
        else:
            break
    tiles = rows // 8
    decay_out = [None] * tiles
    value_out = [None] * tiles
    carry_a = jnp.ones_like(values[:1])
    carry_b = jnp.zeros_like(values[:1])
    for tile in reversed(range(tiles)):
        part_a = decays[tile * 8 : tile * 8 + 8]
        part_b = values[tile * 8 : tile * 8 + 8]
        value_out[tile] = part_b + part_a * carry_b
        decay_out[tile] = part_a * carry_a
        carry_b = value_out[tile][:1]
        carry_a = decay_out[tile][:1]
    return decay_out, value_out


def mixer_kernel(grad_ref, weight_ref, gelu_ref, slope_ref, next_ref, first_ref,
                 gate_ref, local_ref, cumul_ref, ends_ref):
    mixer = jnp.dot(grad_ref[...], weight_ref[...], preferred_element_type=f32)
    gate_ref[...] = (mixer * slope_ref[...]).astype(bf16)
    decays, values = back_scan(next_ref[...], mixer * gelu_ref[...])
    for tile, (part_a, part_b) in enumerate(zip(decays, values)):
        cumul_ref[tile * 8 : tile * 8 + 8] = part_a
        local_ref[tile * 8 : tile * 8 + 8] = part_b
    first = first_ref[...]
    end_a = first * decays[0][:1]
    end_b = first * values[0][:1]
    for peer in range(ends_ref.shape[0]):
        ends_ref[peer] = jnp.concatenate([end_a, end_b], axis=0)


def mixer_call(input_grad, out_weight, gelu, slope, next_decay, first, peers):
    rows, width = input_grad.shape
    channels = out_weight.shape[1]
    block = 256
    wide = pl.BlockSpec((rows, block), lambda i: (0, i))
    return pl.pallas_call(
        mixer_kernel,
        grid=(channels // block,),
        in_specs=[
            pl.BlockSpec((rows, width), lambda i: (0, 0)),
            pl.BlockSpec((width, block), lambda i: (0, i)),
            wide, wide, wide,
            pl.BlockSpec((1, block), lambda i: (0, i)),
        ],
        out_specs=[wide, wide, wide, pl.BlockSpec((peers, 2, block), lambda i: (0, 0, i))],
        out_shape=[
            jax.ShapeDtypeStruct((rows, channels), bf16),
            jax.ShapeDtypeStruct((rows, channels), f32),
            jax.ShapeDtypeStruct((rows, channels), f32),
            jax.ShapeDtypeStruct((peers, 2, channels), f32),
        ],
        cost_estimate=pl.CostEstimate(
            flops=2 * rows * width * channels, bytes_accessed=8 << 20, transcendentals=0
        ),
        name="mixer",
    )(input_grad, out_weight, gelu, slope, next_decay, first)


def tail_kernel(where_ref, ends_ref, local_ref, cumul_ref, to_decay_ref, to_input_ref, direct_ref,
                head_ref, head_coef_ref, taps_ref, decay_w_ref, input_w_ref, out_ref):
    mine = where_ref[0]
    count = ends_ref.shape[0]
    carry = jnp.zeros_like(local_ref[:1])
    head_carry = carry
    for place in reversed(range(1, count)):
        ends = ends_ref[place]
        longer = ends[1:2] + ends[0:1] * carry
        head_carry = jnp.where(place > mine + 1, longer, head_carry)
        carry = jnp.where(place > mine, longer, carry)
    decay_w = decay_w_ref[0]
    input_w = input_w_ref[0]

    def conv_grad(carried, to_decay, to_input, direct):
        decay_pre = (carried * to_decay).astype(bf16)
        input_pre = (carried * to_input).astype(bf16)
        return carried * direct + cols_of(decay_pre, decay_w) + cols_of(input_pre, input_w)

    main = conv_grad(
        local_ref[...] + cumul_ref[...] * carry, to_decay_ref[...], to_input_ref[...], direct_ref[...]
    )
    halo = conv_grad(
        head_ref[...] + head_coef_ref[0] * head_carry,
        head_coef_ref[1], head_coef_ref[2], head_coef_ref[3],
    )
    rows = main.shape[0]
    whole = jnp.concatenate([main, halo], axis=0)
    taps = taps_ref[...].astype(f32)
    total = taps[0:1] * pltpu.roll(whole, whole.shape[0] - 3, 0)
    for tap in range(1, 3):
        total = total + taps[tap : tap + 1] * pltpu.roll(whole, whole.shape[0] - 3 + tap, 0)
    total = total + taps[3:4] * whole
    out_ref[...] = total[:rows].astype(bf16)


def tail_call(mine, ends, local, cumul, to_decay, to_input, direct, head, head_coef, taps, decay_w, input_w):
    rows, channels = local.shape
    count = ends.shape[0]
    block = decay_w.shape[1]
    wide = pl.BlockSpec((rows, block), lambda i, s: (0, i))
    return pl.pallas_call(
        tail_kernel,
        grid_spec=pltpu.PrefetchScalarGridSpec(
            num_scalar_prefetch=1,
            grid=(channels // block,),
            in_specs=[
                pl.BlockSpec((count, 2, block), lambda i, s: (0, 0, i)),
                wide, wide, wide, wide, wide,
                pl.BlockSpec((8, block), lambda i, s: (0, i)),
                pl.BlockSpec((4, 8, block), lambda i, s: (0, 0, i)),
                pl.BlockSpec((4, block), lambda i, s: (0, i)),
                pl.BlockSpec((1, block, block), lambda i, s: (i, 0, 0)),
                pl.BlockSpec((1, block, block), lambda i, s: (i, 0, 0)),
            ],
            out_specs=wide,
        ),
        out_shape=jax.ShapeDtypeStruct((rows, channels), bf16),
        cost_estimate=pl.CostEstimate(
            flops=8 * rows * block * channels, bytes_accessed=7 << 20, transcendentals=0
        ),
        name="tail",
    )(mine, ends, local, cumul, to_decay, to_input, direct, head, head_coef, taps, decay_w, input_w)


def on_device(
    moe_input,
    cotangent,
    expert_ids,
    route_weight,
    gate_proj,
    up_proj,
    down_proj,
    out_weight,
    recur_input,
    gate_input,
    states,
    conv_taps,
    decay_gate_w,
    input_gate_w,
    decay_rate,
    decay_extra,
):
    experts = lax.axis_size("sp")
    cores = lax.axis_size("tp")
    place = lax.axis_index("sp")
    core = lax.axis_index("tp")
    outer = 4 if experts % 4 == 0 else 1
    plane = experts // outer
    tok_rows, width = moe_input.shape
    channels = recur_input.shape[1]
    top_count = expert_ids.shape[1]
    capacity = max(2, 4 * tok_rows // experts)
    share = capacity // cores
    own_slots = experts * share

    flat_ids = expert_ids.reshape(-1)
    onehot = (flat_ids[:, None] == jnp.arange(experts, dtype=jnp.int32)[None, :]).astype(jnp.int32)
    slot_rank = jnp.sum((jnp.cumsum(onehot, axis=0) - onehot) * onehot, axis=1)
    pair_slots = (flat_ids * capacity + slot_rank).reshape(tok_rows, top_count)
    slot_iota = jnp.arange(own_slots, dtype=jnp.int32)
    slot_ids = (slot_iota // share) * capacity + core * share + slot_iota % share
    hits = slot_ids[:, None, None] == pair_slots[None, :, :]
    placing = jnp.any(hits, axis=2).astype(bf16)
    slot_weight = jnp.sum(jnp.where(hits, route_weight[None, :, :], 0.0), axis=(1, 2))
    send_rows = times(placing, moe_input).astype(bf16).reshape(experts, share, width)
    send_grads = (
        (times(placing, cotangent) * slot_weight[:, None]).astype(bf16).reshape(experts, share, width)
    )
    got_rows = lax.all_to_all(send_rows, "sp", split_axis=0, concat_axis=0, tiled=True)
    got_grads = lax.all_to_all(send_grads, "sp", split_axis=0, concat_axis=0, tiled=True)
    rows_here = got_rows.reshape(own_slots, width)
    grads_here = got_grads.reshape(own_slots, width)
    rows_there = swapped(rows_here, "tp", 1)
    grads_there = swapped(grads_here, "tp", 1)

    weight_gate = gate_proj[0]
    weight_up = up_proj[0]
    weight_down = down_proj[0]

    def expert(rows_in, grads_in):
        gate_pre = times(rows_in, weight_gate)
        up_pre = times(rows_in, weight_up)
        sigmoid_gate = jax.nn.sigmoid(gate_pre)
        silu_gate = gate_pre * sigmoid_gate
        hidden = (silu_gate * up_pre).astype(bf16)
        hidden_grad = cols_of(grads_in, weight_down)
        gate_pre_grad = (
            hidden_grad * up_pre * sigmoid_gate * (1.0 + gate_pre * (1.0 - sigmoid_gate))
        ).astype(bf16)
        up_pre_grad = (hidden_grad * silu_gate).astype(bf16)
        partial = cols_of(gate_pre_grad, weight_gate) + cols_of(up_pre_grad, weight_up)
        return hidden, gate_pre_grad, up_pre_grad, partial

    hidden_t, gate_t, up_t, partial_t = expert(rows_there, grads_there)
    from_there = swapped(partial_t.astype(bf16), "tp", 1)
    hidden_h, gate_h, up_h, partial_h = expert(rows_here, grads_here)
    shared = (partial_h + from_there.astype(f32)).astype(bf16).reshape(experts, share, width)
    back = lax.all_to_all(shared, "sp", split_axis=0, concat_axis=0, tiled=True)
    down_grad = rows_of(hidden_h, grads_here) + rows_of(hidden_t, grads_there)
    gate_weight_grad = rows_of(rows_here, gate_h) + rows_of(rows_there, gate_t)
    up_weight_grad = rows_of(rows_here, up_h) + rows_of(rows_there, up_t)

    gate_float = gate_input.astype(f32)
    gelu_value, gelu_back = jax.vjp(jax.nn.gelu, gate_float)
    slope = states * gelu_back(jnp.ones_like(gate_float))[0]
    mixer_out = (states * gelu_value).astype(bf16)
    mixers = [mixer_out] + [swapped(mixer_out, "sp", k) for k in range(1, plane)]
    prev_inputs = shifted(recur_input[-8:], "sp", 1)
    prev_state = shifted(states[-1:], "sp", 1)
    extended = jnp.concatenate([prev_inputs[-3:], recur_input], axis=0).astype(f32)
    taps = conv_taps.astype(f32)
    conv = taps[0] * extended[0:tok_rows]
    for tap in range(1, 4):
        conv = conv + taps[tap] * extended[tap : tap + tok_rows]
    blocks, block_width = decay_gate_w.shape[:2]
    conv_low = conv.astype(bf16)

    def by_block(value, weights):
        parts = [
            times(value[:, b * block_width : (b + 1) * block_width], weights[b]) for b in range(blocks)
        ]
        return jnp.concatenate(parts, axis=1)

    recur_gate = jax.nn.sigmoid(by_block(conv_low, decay_gate_w))
    input_gate = jax.nn.sigmoid(by_block(conv_low, input_gate_w))
    first_row = (place * tok_rows + jnp.arange(tok_rows, dtype=jnp.int32) == 0)[:, None]
    log_decay = -decay_scale * recur_gate * decay_rate[None, :] + decay_extra
    decay_value = jnp.exp(log_decay)
    mult = jnp.where(first_row, 1.0, jnp.sqrt(-jnp.expm1(2.0 * log_decay)))
    prev_states = jnp.concatenate([prev_state, states[:-1]], axis=0)
    next_decay = jnp.concatenate([decay_value[1:], jnp.ones((1, channels), f32)], axis=0)
    to_log = prev_states * decay_value - jnp.where(
        first_row, 0.0, input_gate * conv * decay_value * decay_value / mult
    )
    to_decay = to_log * (-decay_scale * decay_rate[None, :]) * recur_gate * (1.0 - recur_gate)
    to_input = mult * conv * input_gate * (1.0 - input_gate)
    direct = mult * input_gate

    mine_back = rows_of(placing, back.reshape(own_slots, width)).astype(bf16)
    other_back = swapped(mine_back, "tp", 1)
    input_grad = (
        mine_back.astype(f32) + other_back.astype(f32) + cotangent.astype(f32)
    ).astype(bf16)

    out_rows = width // experts
    split_grad = input_grad.reshape(tok_rows, outer, plane, out_rows)
    inner = place % plane

    def columns_for(index):
        part = lax.dynamic_slice_in_dim(split_grad, index, 1, 2)
        return part.reshape(tok_rows, outer * out_rows)

    grads = [columns_for(inner)]
    grads += [swapped(columns_for(inner ^ k), "sp", k) for k in range(1, plane)]
    gate_grad, local, cumul, ends = mixer_call(
        input_grad, out_weight, gelu_value, slope, next_decay, decay_value[:1], experts
    )
    head_coef = jnp.stack([to_decay[:8], to_input[:8], direct[:8]])
    head_coef = shifted(head_coef, "sp", -1)
    head = shifted(jnp.stack([local[:8], cumul[:8]]), "sp", -1)
    ends = lax.all_to_all(ends, "sp", split_axis=0, concat_axis=0, tiled=True)
    product = rows_of(grads[0], mixers[0])
    for k in range(1, plane):
        product = product + rows_of(grads[k], mixers[k])
    product = product.reshape(outer, out_rows, channels)
    level = place // plane

    def block_for(index):
        return lax.dynamic_slice_in_dim(product, index, 1, 0)[0]

    out_weight_grad = block_for(level)
    for k in range(1, outer):
        received = swapped(block_for(level ^ k).astype(bf16), "sp", k * plane)
        out_weight_grad = out_weight_grad + received.astype(f32)

    head_coef = jnp.concatenate([head[1:], head_coef], axis=0)
    recur_grad = tail_call(
        place[None].astype(jnp.int32), ends, local, cumul, to_decay, to_input, direct,
        head[0], head_coef, conv_taps, decay_gate_w, input_gate_w,
    )
    return (
        gate_weight_grad.astype(bf16)[None],
        up_weight_grad.astype(bf16)[None],
        down_grad.astype(bf16)[None],
        out_weight_grad,
        input_grad,
        recur_grad,
        gate_grad,
    )


def solution(mesh):
    return jax.shard_map(
        on_device,
        mesh=mesh,
        in_specs=(
            P("sp", None),
            P("sp", None),
            P("sp", None),
            P("sp", None),
            P("sp", None, "tp"),
            P("sp", None, "tp"),
            P("sp", "tp", None),
            P(None, "tp"),
            P("sp", "tp"),
            P("sp", "tp"),
            P("sp", "tp"),
            P(None, "tp"),
            P("tp", None, None),
            P("tp", None, None),
            P("tp"),
            P("sp", "tp"),
        ),
        out_specs=(
            P("sp", None, "tp"),
            P("sp", None, "tp"),
            P("sp", "tp", None),
            P("sp", "tp"),
            P("sp", None),
            P("sp", "tp"),
            P("sp", "tp"),
        ),
        check_vma=False,
    )
```

```python
import jax
import jax.numpy as jnp
from jax import lax
from jax.experimental import pallas as pl
from jax.experimental.pallas import tpu as pltpu
from jax.sharding import PartitionSpec as P


decay_scale = 8.0
f32 = jnp.float32
bf16 = jnp.bfloat16


def dot(left, right, contract):
    return lax.dot_general(left, right, (contract, ((), ())), preferred_element_type=f32)


def rows_of(left, right):
    return dot(left, right, ((0,), (0,)))


def cols_of(left, right):
    return dot(left, right, ((1,), (1,)))


def times(left, right):
    return dot(left, right, ((1,), (0,)))


def shifted(value, axis, steps):
    count = lax.axis_size(axis)
    pairs = [(s, s + steps) for s in range(max(0, -steps), min(count, count - steps))]
    return lax.ppermute(value, axis, pairs)


def swapped(value, axis, mask):
    count = lax.axis_size(axis)
    return lax.ppermute(value, axis, [(s, s ^ mask) for s in range(count)])


def back_scan(decays, values):
    rows = values.shape[0]
    inner = lax.broadcasted_iota(jnp.int32, values.shape, 0) % 8
    step = 1
    while step < rows:
        if step < 8:
            keep = inner < 8 - step
            later_a = jnp.where(keep, pltpu.roll(decays, rows - step, 0), 1.0)
            later_b = jnp.where(keep, pltpu.roll(values, rows - step, 0), 0.0)
            values = values + decays * later_b
            decays = decays * later_a
            step *= 2
        else:
            break
    tiles = rows // 8
    decay_out = [None] * tiles
    value_out = [None] * tiles
    carry_a = jnp.ones_like(values[:1])
    carry_b = jnp.zeros_like(values[:1])
    for tile in reversed(range(tiles)):
        part_a = decays[tile * 8 : tile * 8 + 8]
        part_b = values[tile * 8 : tile * 8 + 8]
        value_out[tile] = part_b + part_a * carry_b
        decay_out[tile] = part_a * carry_a
        carry_b = value_out[tile][:1]
        carry_a = decay_out[tile][:1]
    return decay_out, value_out


def mixer_kernel(grad_ref, weight_ref, gelu_ref, slope_ref, next_ref, first_ref,
                 gate_ref, local_ref, cumul_ref, ends_ref):
    mixer = jnp.dot(grad_ref[...], weight_ref[...], preferred_element_type=f32)
    gate_ref[...] = (mixer * slope_ref[...]).astype(bf16)
    decays, values = back_scan(next_ref[...], mixer * gelu_ref[...])
    for tile, (part_a, part_b) in enumerate(zip(decays, values)):
        cumul_ref[tile * 8 : tile * 8 + 8] = part_a
        local_ref[tile * 8 : tile * 8 + 8] = part_b
    first = first_ref[...]
    end_a = first * decays[0][:1]
    end_b = first * values[0][:1]
    for peer in range(ends_ref.shape[0]):
        ends_ref[peer] = jnp.concatenate([end_a, end_b], axis=0)


def mixer_call(input_grad, out_weight, gelu, slope, next_decay, first, peers):
    rows, width = input_grad.shape
    channels = out_weight.shape[1]
    block = 256
    wide = pl.BlockSpec((rows, block), lambda i: (0, i))
    return pl.pallas_call(
        mixer_kernel,
        grid=(channels // block,),
        in_specs=[
            pl.BlockSpec((rows, width), lambda i: (0, 0)),
            pl.BlockSpec((width, block), lambda i: (0, i)),
            wide, wide, wide,
            pl.BlockSpec((1, block), lambda i: (0, i)),
        ],
        out_specs=[wide, wide, wide, pl.BlockSpec((peers, 2, block), lambda i: (0, 0, i))],
        out_shape=[
            jax.ShapeDtypeStruct((rows, channels), bf16),
            jax.ShapeDtypeStruct((rows, channels), f32),
            jax.ShapeDtypeStruct((rows, channels), f32),
            jax.ShapeDtypeStruct((peers, 2, channels), f32),
        ],
        cost_estimate=pl.CostEstimate(
            flops=2 * rows * width * channels, bytes_accessed=8 << 20, transcendentals=0
        ),
        name="mixer",
    )(input_grad, out_weight, gelu, slope, next_decay, first)


def tail_kernel(where_ref, ends_ref, local_ref, cumul_ref, to_decay_ref, to_input_ref, direct_ref,
                head_ref, head_coef_ref, taps_ref, decay_w_ref, input_w_ref, out_ref):
    mine = where_ref[0]
    count = ends_ref.shape[0]
    carry = jnp.zeros_like(local_ref[:1])
    head_carry = carry
    for place in reversed(range(1, count)):
        ends = ends_ref[place]
        longer = ends[1:2] + ends[0:1] * carry
        head_carry = jnp.where(place > mine + 1, longer, head_carry)
        carry = jnp.where(place > mine, longer, carry)
    decay_w = decay_w_ref[0]
    input_w = input_w_ref[0]

    def conv_grad(carried, to_decay, to_input, direct):
        decay_pre = (carried * to_decay).astype(bf16)
        input_pre = (carried * to_input).astype(bf16)
        return carried * direct + cols_of(decay_pre, decay_w) + cols_of(input_pre, input_w)

    main = conv_grad(
        local_ref[...] + cumul_ref[...] * carry, to_decay_ref[...], to_input_ref[...], direct_ref[...]
    )
    halo = conv_grad(
        head_ref[...] + head_coef_ref[0] * head_carry,
        head_coef_ref[1], head_coef_ref[2], head_coef_ref[3],
    )
    rows = main.shape[0]
    whole = jnp.concatenate([main, halo], axis=0)
    taps = taps_ref[...].astype(f32)
    total = taps[0:1] * pltpu.roll(whole, whole.shape[0] - 3, 0)
    for tap in range(1, 3):
        total = total + taps[tap : tap + 1] * pltpu.roll(whole, whole.shape[0] - 3 + tap, 0)
    total = total + taps[3:4] * whole
    out_ref[...] = total[:rows].astype(bf16)


def tail_call(mine, ends, local, cumul, to_decay, to_input, direct, head, head_coef, taps, decay_w, input_w):
    rows, channels = local.shape
    count = ends.shape[0]
    block = decay_w.shape[1]
    wide = pl.BlockSpec((rows, block), lambda i, s: (0, i))
    return pl.pallas_call(
        tail_kernel,
        grid_spec=pltpu.PrefetchScalarGridSpec(
            num_scalar_prefetch=1,
            grid=(channels // block,),
            in_specs=[
                pl.BlockSpec((count, 2, block), lambda i, s: (0, 0, i)),
                wide, wide, wide, wide, wide,
                pl.BlockSpec((8, block), lambda i, s: (0, i)),
                pl.BlockSpec((4, 8, block), lambda i, s: (0, 0, i)),
                pl.BlockSpec((4, block), lambda i, s: (0, i)),
                pl.BlockSpec((1, block, block), lambda i, s: (i, 0, 0)),
                pl.BlockSpec((1, block, block), lambda i, s: (i, 0, 0)),
            ],
            out_specs=wide,
        ),
        out_shape=jax.ShapeDtypeStruct((rows, channels), bf16),
        cost_estimate=pl.CostEstimate(
            flops=8 * rows * block * channels, bytes_accessed=7 << 20, transcendentals=0
        ),
        name="tail",
    )(mine, ends, local, cumul, to_decay, to_input, direct, head, head_coef, taps, decay_w, input_w)


def combine_kernel(where_ref, mine_ref, other_ref, cot_ref, grad_ref, *piece_refs):
    total = mine_ref[...].astype(f32) + other_ref[...].astype(f32) + cot_ref[...].astype(f32)
    grad_ref[...] = total.astype(bf16)
    group = len(piece_refs)
    inner = lax.rem(where_ref[0], group)
    wide = grad_ref.shape[1] // group
    cut = piece_refs[0].shape[1]
    lanes = 128
    outer = cut // lanes
    assert wide == cut
    for k, piece_ref in enumerate(piece_refs):
        for level in range(outer):
            column = pl.multiple_of((level * group + (inner ^ k)) * lanes, lanes)
            piece_ref[:, level * lanes : (level + 1) * lanes] = grad_ref[:, pl.ds(column, lanes)]


def combine_call(where, mine, other, cotangent, group):
    rows, width = mine.shape
    block = rows // 4
    cut = width // group
    wide = pl.BlockSpec((block, width), lambda i, s: (i, 0))
    return pl.pallas_call(
        combine_kernel,
        grid_spec=pltpu.PrefetchScalarGridSpec(
            num_scalar_prefetch=1,
            grid=(4,),
            in_specs=[wide, wide, wide],
            out_specs=[wide] + [pl.BlockSpec((block, cut), lambda i, s: (i, 0))] * group,
        ),
        out_shape=[jax.ShapeDtypeStruct((rows, width), bf16)]
        + [jax.ShapeDtypeStruct((rows, cut), bf16)] * group,
        cost_estimate=pl.CostEstimate(flops=1 << 28, bytes_accessed=5 << 20, transcendentals=0),
        name="combine",
    )(where, mine, other, cotangent)


def on_device(
    moe_input,
    cotangent,
    expert_ids,
    route_weight,
    gate_proj,
    up_proj,
    down_proj,
    out_weight,
    recur_input,
    gate_input,
    states,
    conv_taps,
    decay_gate_w,
    input_gate_w,
    decay_rate,
    decay_extra,
):
    experts = lax.axis_size("sp")
    cores = lax.axis_size("tp")
    place = lax.axis_index("sp")
    core = lax.axis_index("tp")
    group = 8 if experts % 8 == 0 else experts
    outer = experts // group
    tok_rows, width = moe_input.shape
    channels = recur_input.shape[1]
    top_count = expert_ids.shape[1]
    capacity = max(2, 4 * tok_rows // experts)
    share = capacity // cores
    own_slots = experts * share

    flat_ids = expert_ids.reshape(-1)
    onehot = (flat_ids[:, None] == jnp.arange(experts, dtype=jnp.int32)[None, :]).astype(jnp.int32)
    slot_rank = jnp.sum((jnp.cumsum(onehot, axis=0) - onehot) * onehot, axis=1)
    pair_slots = (flat_ids * capacity + slot_rank).reshape(tok_rows, top_count)
    slot_iota = jnp.arange(own_slots, dtype=jnp.int32)
    slot_ids = (slot_iota // share) * capacity + core * share + slot_iota % share
    hits = slot_ids[:, None, None] == pair_slots[None, :, :]
    placing = jnp.any(hits, axis=2).astype(bf16)
    slot_weight = jnp.sum(jnp.where(hits, route_weight[None, :, :], 0.0), axis=(1, 2))
    send_rows = times(placing, moe_input).astype(bf16).reshape(experts, share, width)
    edge = jnp.concatenate([recur_input[-3:].astype(f32), states[-1:]], axis=0)
    edge = shifted(edge, "sp", 1)
    edge, send_rows, late = lax.optimization_barrier((edge, send_rows, (gate_input, states, cotangent)))
    gate_input, states, cotangent_late = late
    got_rows = lax.all_to_all(send_rows, "sp", split_axis=0, concat_axis=0, tiled=True)

    send_grads = times(placing, cotangent_late) * slot_weight[:, None]
    send_grads = send_grads.astype(bf16).reshape(experts, share, width)

    gate_float = gate_input.astype(f32)
    gelu_value, gelu_back = jax.vjp(jax.nn.gelu, gate_float)
    slope = states * gelu_back(jnp.ones_like(gate_float))[0]
    mixer_out = (states * gelu_value).astype(bf16)
    extended = jnp.concatenate([edge[:3], recur_input.astype(f32)], axis=0)
    prev_state = edge[3:]
    taps = conv_taps.astype(f32)
    conv = taps[0] * extended[0:tok_rows]
    for tap in range(1, 4):
        conv = conv + taps[tap] * extended[tap : tap + tok_rows]
    blocks, block_width = decay_gate_w.shape[:2]
    conv_low = conv.astype(bf16)

    def by_block(value, weights):
        parts = [
            times(value[:, b * block_width : (b + 1) * block_width], weights[b]) for b in range(blocks)
        ]
        return jnp.concatenate(parts, axis=1)

    recur_gate = jax.nn.sigmoid(by_block(conv_low, decay_gate_w))
    input_gate = jax.nn.sigmoid(by_block(conv_low, input_gate_w))
    first_row = (place * tok_rows + jnp.arange(tok_rows, dtype=jnp.int32) == 0)[:, None]
    log_decay = -decay_scale * recur_gate * decay_rate[None, :] + decay_extra
    decay_value = jnp.exp(log_decay)
    mult = jnp.where(first_row, 1.0, jnp.sqrt(-jnp.expm1(2.0 * log_decay)))
    prev_states = jnp.concatenate([prev_state, states[:-1]], axis=0)
    next_decay = jnp.concatenate([decay_value[1:], jnp.ones((1, channels), f32)], axis=0)
    to_log = prev_states * decay_value - jnp.where(
        first_row, 0.0, input_gate * conv * decay_value * decay_value / mult
    )
    to_decay = to_log * (-decay_scale * decay_rate[None, :]) * recur_gate * (1.0 - recur_gate)
    to_input = mult * conv * input_gate * (1.0 - input_gate)
    direct = mult * input_gate

    statics = (gelu_value, slope, mixer_out, next_decay, decay_value[:1], to_decay, to_input, direct)
    statics, send_grads = lax.optimization_barrier((statics, send_grads))
    gelu_value, slope, mixer_out, next_decay, first_decay, to_decay, to_input, direct = statics

    got_grads = lax.all_to_all(send_grads, "sp", split_axis=0, concat_axis=0, tiled=True)
    rows_here = got_rows.reshape(own_slots, width)
    rows_there = swapped(rows_here, "tp", 1)
    head_coef = shifted(jnp.stack([to_decay[:8], to_input[:8], direct[:8]]), "sp", -1)
    mixers = {0: mixer_out}
    half = group // 2
    mixers[half] = swapped(mixer_out, "sp", half)
    weight_gate = gate_proj[0]
    weight_up = up_proj[0]
    weight_down = down_proj[0]
    pres = tuple(
        (times(rows, weight_gate), times(rows, weight_up)) for rows in (rows_here, rows_there)
    )
    got_grads, mixers[half], pres, rows_there = lax.optimization_barrier(
        (got_grads, mixers[half], pres, rows_there)
    )
    for k in range(1, half):
        mixers[k] = swapped(mixer_out, "sp", k)
        mixers[k ^ half] = swapped(mixers[half], "sp", k)
    grads_here = got_grads.reshape(own_slots, width)
    grads_there = swapped(grads_here, "tp", 1)

    def expert(pre, grads_in):
        gate_pre, up_pre = pre
        sigmoid_gate = jax.nn.sigmoid(gate_pre)
        silu_gate = gate_pre * sigmoid_gate
        hidden = (silu_gate * up_pre).astype(bf16)
        hidden_grad = cols_of(grads_in, weight_down)
        gate_pre_grad = (
            hidden_grad * up_pre * sigmoid_gate * (1.0 + gate_pre * (1.0 - sigmoid_gate))
        ).astype(bf16)
        up_pre_grad = (hidden_grad * silu_gate).astype(bf16)
        return hidden, gate_pre_grad, up_pre_grad

    hidden_h, gate_h, up_h = expert(pres[0], grads_here)
    grads_there, hidden_h, gate_h, up_h = lax.optimization_barrier((grads_there, hidden_h, gate_h, up_h))
    hidden_t, gate_t, up_t = expert(pres[1], grads_there)
    partial_t = cols_of(gate_t, weight_gate) + cols_of(up_t, weight_up)
    from_there = swapped(partial_t.astype(bf16), "tp", 1)
    partial_h = cols_of(gate_h, weight_gate) + cols_of(up_h, weight_up)
    shared = (partial_h + from_there.astype(f32)).astype(bf16).reshape(experts, share, width)
    back = lax.all_to_all(shared, "sp", split_axis=0, concat_axis=0, tiled=True)
    down_grad = rows_of(hidden_h, grads_here) + rows_of(hidden_t, grads_there)
    gate_weight_grad = rows_of(rows_here, gate_h) + rows_of(rows_there, gate_t)
    up_weight_grad = rows_of(rows_here, up_h) + rows_of(rows_there, up_t)
    weight_grads = (gate_weight_grad.astype(bf16), up_weight_grad.astype(bf16), down_grad.astype(bf16))
    back, weight_grads, mixers, head_coef = lax.optimization_barrier(
        (back, weight_grads, mixers, head_coef)
    )

    mine_back = rows_of(placing, back.reshape(own_slots, width)).astype(bf16)
    other_back = swapped(mine_back, "tp", 1)
    out_rows = width // experts
    where = place[None].astype(jnp.int32)
    if out_rows % 128 == 0:
        input_grad, *pieces = combine_call(where, mine_back, other_back, cotangent, group)
    else:
        input_grad = (
            mine_back.astype(f32) + other_back.astype(f32) + cotangent.astype(f32)
        ).astype(bf16)
        split_grad = input_grad.reshape(tok_rows, outer, group, out_rows)
        pieces = [
            lax.dynamic_slice_in_dim(split_grad, place % group ^ k, 1, 2).reshape(tok_rows, -1)
            for k in range(group)
        ]

    grads = [pieces[0]]
    for k in range(1, group):
        grads.append(swapped(pieces[k], "sp", k))
    gate_grad, local, cumul, ends = mixer_call(
        input_grad, out_weight, gelu_value, slope, next_decay, first_decay, experts
    )
    head = shifted(jnp.stack([local[:8], cumul[:8]]), "sp", -1)
    ends = lax.all_to_all(ends, "sp", split_axis=0, concat_axis=0, tiled=True)
    grads, ends, head = lax.optimization_barrier((grads, ends, head))
    product = rows_of(grads[0], mixers[0])
    for k in range(1, group):
        product = product + rows_of(grads[k], mixers[k])
    product = product.reshape(outer, out_rows, channels)
    level = place // group

    def block_for(index):
        return lax.dynamic_slice_in_dim(product, index, 1, 0)[0]

    out_weight_grad = block_for(level)
    for k in range(1, outer):
        received = swapped(block_for(level ^ k).astype(bf16), "sp", k * group)
        out_weight_grad = out_weight_grad + received.astype(f32)

    head_coef = jnp.concatenate([head[1:], head_coef], axis=0)
    recur_grad = tail_call(
        where, ends, local, cumul, to_decay, to_input, direct,
        head[0], head_coef, conv_taps, decay_gate_w, input_gate_w,
    )
    return (
        weight_grads[0][None],
        weight_grads[1][None],
        weight_grads[2][None],
        out_weight_grad,
        input_grad,
        recur_grad,
        gate_grad,
    )


def solution(mesh):
    return jax.shard_map(
        on_device,
        mesh=mesh,
        in_specs=(
            P("sp", None),
            P("sp", None),
            P("sp", None),
            P("sp", None),
            P("sp", None, "tp"),
            P("sp", None, "tp"),
            P("sp", "tp", None),
            P(None, "tp"),
            P("sp", "tp"),
            P("sp", "tp"),
            P("sp", "tp"),
            P(None, "tp"),
            P("tp", None, None),
            P("tp", None, None),
            P("tp"),
            P("sp", "tp"),
        ),
        out_specs=(
            P("sp", None, "tp"),
            P("sp", None, "tp"),
            P("sp", "tp", None),
            P("sp", "tp"),
            P("sp", None),
            P("sp", "tp"),
            P("sp", "tp"),
        ),
        check_vma=False,
    )
```

```python
import functools

import jax
import jax.numpy as jnp
from jax import lax
from jax.experimental import pallas as pl
from jax.experimental.pallas import tpu as pltpu
from jax.sharding import PartitionSpec as P


decay_scale = 8.0
f32 = jnp.float32
bf16 = jnp.bfloat16


def dot(left, right, contract):
    return lax.dot_general(left, right, (contract, ((), ())), preferred_element_type=f32)


def rows_of(left, right):
    return dot(left, right, ((0,), (0,)))


def cols_of(left, right):
    return dot(left, right, ((1,), (1,)))


def times(left, right):
    return dot(left, right, ((1,), (0,)))


def shifted(value, axis, steps):
    count = lax.axis_size(axis)
    pairs = [(s, s + steps) for s in range(max(0, -steps), min(count, count - steps))]
    return lax.ppermute(value, axis, pairs)


def swapped(value, axis, mask):
    count = lax.axis_size(axis)
    return lax.ppermute(value, axis, [(s, s ^ mask) for s in range(count)])


def back_scan(decays, values):
    rows = values.shape[0]
    inner = lax.broadcasted_iota(jnp.int32, values.shape, 0) % 8
    step = 1
    while step < rows:
        if step < 8:
            keep = inner < 8 - step
            later_a = jnp.where(keep, pltpu.roll(decays, rows - step, 0), 1.0)
            later_b = jnp.where(keep, pltpu.roll(values, rows - step, 0), 0.0)
            values = values + decays * later_b
            decays = decays * later_a
            step *= 2
        else:
            break
    tiles = rows // 8
    decay_out = [None] * tiles
    value_out = [None] * tiles
    carry_a = jnp.ones_like(values[:1])
    carry_b = jnp.zeros_like(values[:1])
    for tile in reversed(range(tiles)):
        part_a = decays[tile * 8 : tile * 8 + 8]
        part_b = values[tile * 8 : tile * 8 + 8]
        value_out[tile] = part_b + part_a * carry_b
        decay_out[tile] = part_a * carry_a
        carry_b = value_out[tile][:1]
        carry_a = decay_out[tile][:1]
    return decay_out, value_out


def mixer_kernel(grad_ref, weight_ref, gelu_ref, slope_ref, next_ref, first_ref,
                 gate_ref, local_ref, cumul_ref, ends_ref):
    mixer = jnp.dot(grad_ref[...], weight_ref[...], preferred_element_type=f32)
    gate_ref[...] = (mixer * slope_ref[...]).astype(bf16)
    decays, values = back_scan(next_ref[...], mixer * gelu_ref[...])
    for tile, (part_a, part_b) in enumerate(zip(decays, values)):
        cumul_ref[tile * 8 : tile * 8 + 8] = part_a
        local_ref[tile * 8 : tile * 8 + 8] = part_b
    first = first_ref[...]
    end_a = first * decays[0][:1]
    end_b = first * values[0][:1]
    for peer in range(ends_ref.shape[0]):
        ends_ref[peer] = jnp.concatenate([end_a, end_b], axis=0)


def mixer_call(input_grad, out_weight, gelu, slope, next_decay, first, peers):
    rows, width = input_grad.shape
    channels = out_weight.shape[1]
    block = 256
    wide = pl.BlockSpec((rows, block), lambda i: (0, i))
    return pl.pallas_call(
        mixer_kernel,
        grid=(channels // block,),
        in_specs=[
            pl.BlockSpec((rows, width), lambda i: (0, 0)),
            pl.BlockSpec((width, block), lambda i: (0, i)),
            wide, wide, wide,
            pl.BlockSpec((1, block), lambda i: (0, i)),
        ],
        out_specs=[wide, wide, wide, pl.BlockSpec((peers, 2, block), lambda i: (0, 0, i))],
        out_shape=[
            jax.ShapeDtypeStruct((rows, channels), bf16),
            jax.ShapeDtypeStruct((rows, channels), f32),
            jax.ShapeDtypeStruct((rows, channels), f32),
            jax.ShapeDtypeStruct((peers, 2, channels), f32),
        ],
        cost_estimate=pl.CostEstimate(
            flops=2 * rows * width * channels, bytes_accessed=8 << 20, transcendentals=0
        ),
        name="mixer",
    )(input_grad, out_weight, gelu, slope, next_decay, first)


def tail_kernel(where_ref, ends_ref, local_ref, cumul_ref, to_decay_ref, to_input_ref, direct_ref,
                head_ref, head_coef_ref, taps_ref, decay_w_ref, input_w_ref, out_ref):
    mine = where_ref[0]
    count = ends_ref.shape[0]
    carry = jnp.zeros_like(local_ref[:1])
    head_carry = carry
    for place in reversed(range(1, count)):
        ends = ends_ref[place]
        longer = ends[1:2] + ends[0:1] * carry
        head_carry = jnp.where(place > mine + 1, longer, head_carry)
        carry = jnp.where(place > mine, longer, carry)
    decay_w = decay_w_ref[0]
    input_w = input_w_ref[0]

    def conv_grad(carried, to_decay, to_input, direct):
        decay_pre = (carried * to_decay).astype(bf16)
        input_pre = (carried * to_input).astype(bf16)
        return carried * direct + cols_of(decay_pre, decay_w) + cols_of(input_pre, input_w)

    main = conv_grad(
        local_ref[...] + cumul_ref[...] * carry, to_decay_ref[...], to_input_ref[...], direct_ref[...]
    )
    halo = conv_grad(
        head_ref[...] + head_coef_ref[0] * head_carry,
        head_coef_ref[1], head_coef_ref[2], head_coef_ref[3],
    )
    rows = main.shape[0]
    whole = jnp.concatenate([main, halo], axis=0)
    taps = taps_ref[...].astype(f32)
    total = taps[0:1] * pltpu.roll(whole, whole.shape[0] - 3, 0)
    for tap in range(1, 3):
        total = total + taps[tap : tap + 1] * pltpu.roll(whole, whole.shape[0] - 3 + tap, 0)
    total = total + taps[3:4] * whole
    out_ref[...] = total[:rows].astype(bf16)


def tail_call(mine, ends, local, cumul, to_decay, to_input, direct, head, head_coef, taps, decay_w, input_w):
    rows, channels = local.shape
    count = ends.shape[0]
    block = decay_w.shape[1]
    wide = pl.BlockSpec((rows, block), lambda i, s: (0, i))
    return pl.pallas_call(
        tail_kernel,
        grid_spec=pltpu.PrefetchScalarGridSpec(
            num_scalar_prefetch=1,
            grid=(channels // block,),
            in_specs=[
                pl.BlockSpec((count, 2, block), lambda i, s: (0, 0, i)),
                wide, wide, wide, wide, wide,
                pl.BlockSpec((8, block), lambda i, s: (0, i)),
                pl.BlockSpec((4, 8, block), lambda i, s: (0, 0, i)),
                pl.BlockSpec((4, block), lambda i, s: (0, i)),
                pl.BlockSpec((1, block, block), lambda i, s: (i, 0, 0)),
                pl.BlockSpec((1, block, block), lambda i, s: (i, 0, 0)),
            ],
            out_specs=wide,
        ),
        out_shape=jax.ShapeDtypeStruct((rows, channels), bf16),
        cost_estimate=pl.CostEstimate(
            flops=8 * rows * block * channels, bytes_accessed=7 << 20, transcendentals=0
        ),
        name="tail",
    )(mine, ends, local, cumul, to_decay, to_input, direct, head, head_coef, taps, decay_w, input_w)


def combine_kernel(lanes, mine_ref, other_ref, cot_ref, grad_ref, piece_ref):
    total = mine_ref[...].astype(f32) + other_ref[...].astype(f32) + cot_ref[...].astype(f32)
    total = total.astype(bf16)
    grad_ref[...] = total
    group, _, cut = piece_ref.shape
    for peer in range(group):
        for level in range(cut // lanes):
            column = (level * group + peer) * lanes
            piece_ref[peer, :, level * lanes : (level + 1) * lanes] = total[:, column : column + lanes]


def combine_call(mine, other, cotangent, group, lanes):
    rows, width = mine.shape
    block = rows // 4
    cut = width // group
    wide = pl.BlockSpec((block, width), lambda i: (i, 0))
    return pl.pallas_call(
        functools.partial(combine_kernel, lanes),
        grid=(4,),
        in_specs=[wide, wide, wide],
        out_specs=[wide, pl.BlockSpec((group, block, cut), lambda i: (0, i, 0))],
        out_shape=[
            jax.ShapeDtypeStruct((rows, width), bf16),
            jax.ShapeDtypeStruct((group, rows, cut), bf16),
        ],
        cost_estimate=pl.CostEstimate(flops=1 << 28, bytes_accessed=5 << 20, transcendentals=0),
        name="combine",
    )(mine, other, cotangent)


def product_kernel(level_ref, *refs):
    count = len(refs) // 2
    out_refs = refs[2 * count :]
    total = rows_of(refs[0][0], refs[count][...])
    for k in range(1, count):
        total = total + rows_of(refs[k][0], refs[count + k][...])
    full_ref = out_refs[0]
    full_ref[...] = total


def product_call(where, grads, mixers):
    group, rows, cut = grads.shape
    channels = mixers[0].shape[1]
    block = channels // 4

    def grad_spec(k):
        return pl.BlockSpec((1, rows, cut), lambda i, s: (jnp.bitwise_xor(lax.rem(s[0], group), k), 0, 0))

    return pl.pallas_call(
        product_kernel,
        grid_spec=pltpu.PrefetchScalarGridSpec(
            num_scalar_prefetch=1,
            grid=(channels // block,),
            in_specs=[grad_spec(k) for k in range(group)]
            + [pl.BlockSpec((rows, block), lambda i, s: (0, i))] * group,
            out_specs=[pl.BlockSpec((cut, block), lambda i, s: (0, i))],
        ),
        out_shape=[jax.ShapeDtypeStruct((cut, channels), f32)],
        cost_estimate=pl.CostEstimate(
            flops=2 * group * rows * cut * channels, bytes_accessed=6 << 20, transcendentals=0
        ),
        name="product",
    )(where, *([grads] * group), *mixers)[0]


def on_device(
    moe_input,
    cotangent,
    expert_ids,
    route_weight,
    gate_proj,
    up_proj,
    down_proj,
    out_weight,
    recur_input,
    gate_input,
    states,
    conv_taps,
    decay_gate_w,
    input_gate_w,
    decay_rate,
    decay_extra,
):
    experts = lax.axis_size("sp")
    cores = lax.axis_size("tp")
    place = lax.axis_index("sp")
    core = lax.axis_index("tp")
    group = 8 if experts % 8 == 0 else experts
    outer = experts // group
    tok_rows, width = moe_input.shape
    channels = recur_input.shape[1]
    top_count = expert_ids.shape[1]
    capacity = max(2, 4 * tok_rows // experts)
    share = capacity // cores
    own_slots = experts * share

    flat_ids = expert_ids.reshape(-1)
    onehot = (flat_ids[:, None] == jnp.arange(experts, dtype=jnp.int32)[None, :]).astype(jnp.int32)
    slot_rank = jnp.sum((jnp.cumsum(onehot, axis=0) - onehot) * onehot, axis=1)
    pair_slots = (flat_ids * capacity + slot_rank).reshape(tok_rows, top_count)
    slot_iota = jnp.arange(own_slots, dtype=jnp.int32)
    slot_ids = (slot_iota // share) * capacity + core * share + slot_iota % share
    hits = slot_ids[:, None, None] == pair_slots[None, :, :]
    placing = jnp.any(hits, axis=2).astype(bf16)
    send_rows = times(placing, moe_input).astype(bf16).reshape(experts, share, width)
    late = (gate_input, states, recur_input, cotangent, route_weight)
    send_rows, late = lax.optimization_barrier((send_rows, late))
    gate_input, states, recur_input, cotangent_late, route_weight = late
    got_rows = lax.all_to_all(send_rows, "sp", split_axis=0, concat_axis=0, tiled=True)
    edge = jnp.concatenate([recur_input[-3:].astype(f32), states[-1:]], axis=0)
    edge = shifted(edge, "sp", 1)
    slot_weight = jnp.sum(jnp.where(hits, route_weight[None, :, :], 0.0), axis=(1, 2))
    send_grads = times(placing, cotangent_late) * slot_weight[:, None]
    send_grads = send_grads.astype(bf16).reshape(experts, share, width)

    gate_float = gate_input.astype(f32)
    gelu_value, gelu_back = jax.vjp(jax.nn.gelu, gate_float)
    slope = states * gelu_back(jnp.ones_like(gate_float))[0]
    mixer_out = (states * gelu_value).astype(bf16)
    half = group // 2
    mixers = {0: mixer_out}
    mixers[half] = swapped(mixer_out, "sp", half)
    for k in range(1, half):
        mixers[k] = swapped(mixer_out, "sp", k)
    send_grads, mixers[half], gelu_value, slope, edge, got_rows = lax.optimization_barrier(
        (send_grads, mixers[half], gelu_value, slope, edge, got_rows)
    )
    got_grads = lax.all_to_all(send_grads, "sp", split_axis=0, concat_axis=0, tiled=True)
    for k in range(1, half):
        mixers[k ^ half] = swapped(mixers[half], "sp", k)
    extended = jnp.concatenate([edge[:3], recur_input.astype(f32)], axis=0)
    prev_state = edge[3:]
    taps = conv_taps.astype(f32)
    conv = taps[0] * extended[0:tok_rows]
    for tap in range(1, 4):
        conv = conv + taps[tap] * extended[tap : tap + tok_rows]
    blocks, block_width = decay_gate_w.shape[:2]
    conv_low = conv.astype(bf16)

    def by_block(value, weights):
        parts = [
            times(value[:, b * block_width : (b + 1) * block_width], weights[b]) for b in range(blocks)
        ]
        return jnp.concatenate(parts, axis=1)

    recur_gate = jax.nn.sigmoid(by_block(conv_low, decay_gate_w))
    input_gate = jax.nn.sigmoid(by_block(conv_low, input_gate_w))
    first_row = (place * tok_rows + jnp.arange(tok_rows, dtype=jnp.int32) == 0)[:, None]
    log_decay = -decay_scale * recur_gate * decay_rate[None, :] + decay_extra
    decay_value = jnp.exp(log_decay)
    mult = jnp.where(first_row, 1.0, jnp.sqrt(-jnp.expm1(2.0 * log_decay)))
    prev_states = jnp.concatenate([prev_state, states[:-1]], axis=0)
    next_decay = jnp.concatenate([decay_value[1:], jnp.ones((1, channels), f32)], axis=0)
    to_log = prev_states * decay_value - jnp.where(
        first_row, 0.0, input_gate * conv * decay_value * decay_value / mult
    )
    to_decay = to_log * (-decay_scale * decay_rate[None, :]) * recur_gate * (1.0 - recur_gate)
    to_input = mult * conv * input_gate * (1.0 - input_gate)
    direct = mult * input_gate

    rows_here = got_rows.reshape(own_slots, width)
    rows_there = swapped(rows_here, "tp", 1)
    weight_gate = gate_proj[0]
    weight_up = up_proj[0]
    weight_down = down_proj[0]
    pres = tuple(
        (times(rows, weight_gate), times(rows, weight_up)) for rows in (rows_here, rows_there)
    )
    gates = (next_decay, decay_value[:1], to_decay, to_input, direct)
    got_grads, mixers, pres, rows_there, gates = lax.optimization_barrier(
        (got_grads, mixers, pres, rows_there, gates)
    )
    next_decay, first_decay, to_decay, to_input, direct = gates
    grads_here = got_grads.reshape(own_slots, width)
    grads_there = swapped(grads_here, "tp", 1)

    def expert(pre, grads_in):
        gate_pre, up_pre = pre
        sigmoid_gate = jax.nn.sigmoid(gate_pre)
        silu_gate = gate_pre * sigmoid_gate
        hidden = (silu_gate * up_pre).astype(bf16)
        hidden_grad = cols_of(grads_in, weight_down)
        gate_pre_grad = (
            hidden_grad * up_pre * sigmoid_gate * (1.0 + gate_pre * (1.0 - sigmoid_gate))
        ).astype(bf16)
        up_pre_grad = (hidden_grad * silu_gate).astype(bf16)
        return hidden, gate_pre_grad, up_pre_grad

    hidden_h, gate_h, up_h = expert(pres[0], grads_here)
    grads_there, hidden_h, gate_h, up_h = lax.optimization_barrier((grads_there, hidden_h, gate_h, up_h))
    hidden_t, gate_t, up_t = expert(pres[1], grads_there)
    partial_t = cols_of(gate_t, weight_gate) + cols_of(up_t, weight_up)
    from_there = swapped(partial_t.astype(bf16), "tp", 1)
    partial_h = cols_of(gate_h, weight_gate) + cols_of(up_h, weight_up)
    shared = (partial_h + from_there.astype(f32)).astype(bf16).reshape(experts, share, width)
    back = lax.all_to_all(shared, "sp", split_axis=0, concat_axis=0, tiled=True)
    head_coef = shifted(jnp.stack([to_decay[:8], to_input[:8], direct[:8]]), "sp", -1)
    down_grad = rows_of(hidden_h, grads_here) + rows_of(hidden_t, grads_there)
    gate_weight_grad = rows_of(rows_here, gate_h) + rows_of(rows_there, gate_t)
    up_weight_grad = rows_of(rows_here, up_h) + rows_of(rows_there, up_t)
    weight_grads = (gate_weight_grad.astype(bf16), up_weight_grad.astype(bf16), down_grad.astype(bf16))
    back, weight_grads, head_coef = lax.optimization_barrier((back, weight_grads, head_coef))

    mine_back = rows_of(placing, back.reshape(own_slots, width)).astype(bf16)
    other_back = swapped(mine_back, "tp", 1)
    out_rows = width // experts
    where = place[None].astype(jnp.int32)
    input_grad, pieces = combine_call(mine_back, other_back, cotangent, group, out_rows)

    groups = [[base + peer for peer in range(group)] for base in range(0, experts, group)]
    grads = lax.all_to_all(
        pieces, "sp", split_axis=0, concat_axis=0, tiled=True, axis_index_groups=groups
    )
    gate_grad, local, cumul, ends = mixer_call(
        input_grad, out_weight, gelu_value, slope, next_decay, first_decay, experts
    )
    head = shifted(jnp.stack([local[:8], cumul[:8]]), "sp", -1)
    ends = lax.all_to_all(ends, "sp", split_axis=0, concat_axis=0, tiled=True)
    product = product_call(where, grads, [mixers[k] for k in range(group)])
    product = product.reshape(outer, out_rows, channels)
    level = place // group

    def block_for(index):
        return lax.dynamic_slice_in_dim(product, index, 1, 0)[0]

    out_weight_grad = block_for(level)
    for k in range(1, outer):
        received = swapped(block_for(level ^ k).astype(bf16), "sp", k * group)
        out_weight_grad = out_weight_grad + received.astype(f32)

    head_coef = jnp.concatenate([head[1:], head_coef], axis=0)
    recur_grad = tail_call(
        where, ends, local, cumul, to_decay, to_input, direct,
        head[0], head_coef, conv_taps, decay_gate_w, input_gate_w,
    )
    return (
        weight_grads[0][None],
        weight_grads[1][None],
        weight_grads[2][None],
        out_weight_grad,
        input_grad,
        recur_grad,
        gate_grad,
    )


def solution(mesh):
    return jax.shard_map(
        on_device,
        mesh=mesh,
        in_specs=(
            P("sp", None),
            P("sp", None),
            P("sp", None),
            P("sp", None),
            P("sp", None, "tp"),
            P("sp", None, "tp"),
            P("sp", "tp", None),
            P(None, "tp"),
            P("sp", "tp"),
            P("sp", "tp"),
            P("sp", "tp"),
            P(None, "tp"),
            P("tp", None, None),
            P("tp", None, None),
            P("tp"),
            P("sp", "tp"),
        ),
        out_specs=(
            P("sp", None, "tp"),
            P("sp", None, "tp"),
            P("sp", "tp", None),
            P("sp", "tp"),
            P("sp", None),
            P("sp", "tp"),
            P("sp", "tp"),
        ),
        check_vma=False,
    )
```

```python
import functools

import jax
import jax.numpy as jnp
from jax import lax
from jax.experimental import pallas as pl
from jax.experimental.pallas import tpu as pltpu
from jax.sharding import PartitionSpec as P


decay_scale = 8.0
f32 = jnp.float32
bf16 = jnp.bfloat16


def dot(left, right, contract):
    return lax.dot_general(left, right, (contract, ((), ())), preferred_element_type=f32)


def rows_of(left, right):
    return dot(left, right, ((0,), (0,)))


def cols_of(left, right):
    return dot(left, right, ((1,), (1,)))


def times(left, right):
    return dot(left, right, ((1,), (0,)))


def shifted(value, axis, steps):
    count = lax.axis_size(axis)
    pairs = [(s, s + steps) for s in range(max(0, -steps), min(count, count - steps))]
    return lax.ppermute(value, axis, pairs)


def swapped(value, axis, mask):
    count = lax.axis_size(axis)
    return lax.ppermute(value, axis, [(s, s ^ mask) for s in range(count)])


def back_scan(decays, values):
    rows = values.shape[0]
    inner = lax.broadcasted_iota(jnp.int32, values.shape, 0) % 8
    step = 1
    while step < rows:
        if step < 8:
            keep = inner < 8 - step
            later_a = jnp.where(keep, pltpu.roll(decays, rows - step, 0), 1.0)
            later_b = jnp.where(keep, pltpu.roll(values, rows - step, 0), 0.0)
            values = values + decays * later_b
            decays = decays * later_a
            step *= 2
        else:
            break
    tiles = rows // 8
    decay_out = [None] * tiles
    value_out = [None] * tiles
    carry_a = jnp.ones_like(values[:1])
    carry_b = jnp.zeros_like(values[:1])
    for tile in reversed(range(tiles)):
        part_a = decays[tile * 8 : tile * 8 + 8]
        part_b = values[tile * 8 : tile * 8 + 8]
        value_out[tile] = part_b + part_a * carry_b
        decay_out[tile] = part_a * carry_a
        carry_b = value_out[tile][:1]
        carry_a = decay_out[tile][:1]
    return decay_out, value_out


def held(count):
    return [pl.BlockSpec(memory_space=pltpu.VMEM)] * count


def params(mib):
    return pltpu.CompilerParams(vmem_limit_bytes=mib << 20)


def mixer_kernel(block, grad_ref, weight_ref, gelu_ref, slope_ref, next_ref, first_ref,
                 gate_ref, local_ref, cumul_ref, ends_ref, head_ref):
    def turn(index, _):
        cols = pl.ds(pl.multiple_of(index * block, block), block)
        mixer = jnp.dot(grad_ref[...], weight_ref[:, cols], preferred_element_type=f32)
        gate_ref[:, cols] = (mixer * slope_ref[:, cols]).astype(bf16)
        decays, values = back_scan(next_ref[:, cols], mixer * gelu_ref[:, cols])
        for tile, (part_a, part_b) in enumerate(zip(decays, values)):
            cumul_ref[tile * 8 : tile * 8 + 8, cols] = part_a
            local_ref[tile * 8 : tile * 8 + 8, cols] = part_b
        head_ref[0, :, cols] = values[0]
        head_ref[1, :, cols] = decays[0]
        first = first_ref[:, cols]
        both = jnp.concatenate([first * decays[0][:1], first * values[0][:1]], axis=0)
        for peer in range(ends_ref.shape[0]):
            ends_ref[peer, :, cols] = both
        return 0

    lax.fori_loop(0, weight_ref.shape[1] // block, turn, 0)


def mixer_call(input_grad, out_weight, gelu, slope, next_decay, first, peers):
    rows, width = input_grad.shape
    channels = out_weight.shape[1]
    return pl.pallas_call(
        functools.partial(mixer_kernel, 256),
        in_specs=held(6),
        out_specs=held(5),
        out_shape=[
            jax.ShapeDtypeStruct((rows, channels), bf16),
            jax.ShapeDtypeStruct((rows, channels), f32),
            jax.ShapeDtypeStruct((rows, channels), f32),
            jax.ShapeDtypeStruct((peers, 2, channels), f32),
            jax.ShapeDtypeStruct((2, 8, channels), f32),
        ],
        compiler_params=params(20),
        cost_estimate=pl.CostEstimate(
            flops=2 * rows * width * channels, bytes_accessed=8 << 20, transcendentals=0
        ),
        name="mixer",
    )(input_grad, out_weight, gelu, slope, next_decay, first)


def tail_kernel(where_ref, ends_ref, local_ref, cumul_ref, to_decay_ref, to_input_ref, direct_ref,
                head_ref, head_coef_ref, taps_ref, decay_w_ref, input_w_ref, out_ref):
    mine = where_ref[0]
    count = ends_ref.shape[0]
    block = decay_w_ref.shape[1]
    rows = local_ref.shape[0]
    taps = taps_ref[...].astype(f32)

    carry = jnp.zeros_like(local_ref[:1])
    head_carry = carry
    for place in reversed(range(1, count)):
        ends = ends_ref[place]
        longer = ends[1:2] + ends[0:1] * carry
        head_carry = jnp.where(place > mine + 1, longer, head_carry)
        carry = jnp.where(place > mine, longer, carry)

    for index in range(decay_w_ref.shape[0]):
        cols = slice(index * block, (index + 1) * block)
        decay_w = decay_w_ref[index]
        input_w = input_w_ref[index]

        def conv_grad(carried, to_decay, to_input, direct):
            decay_pre = (carried * to_decay).astype(bf16)
            input_pre = (carried * to_input).astype(bf16)
            return carried * direct + cols_of(decay_pre, decay_w) + cols_of(input_pre, input_w)

        main = conv_grad(
            local_ref[:, cols] + cumul_ref[:, cols] * carry[:, cols],
            to_decay_ref[:, cols], to_input_ref[:, cols], direct_ref[:, cols],
        )
        halo = conv_grad(
            head_ref[0, :, cols] + head_ref[1, :, cols] * head_carry[:, cols],
            head_coef_ref[0, :, cols], head_coef_ref[1, :, cols], head_coef_ref[2, :, cols],
        )
        whole = jnp.concatenate([main, halo], axis=0)
        total = taps[0:1, cols] * pltpu.roll(whole, whole.shape[0] - 3, 0)
        for tap in range(1, 3):
            total = total + taps[tap : tap + 1, cols] * pltpu.roll(whole, whole.shape[0] - 3 + tap, 0)
        total = total + taps[3:4, cols] * whole
        out_ref[:, cols] = total[:rows].astype(bf16)


def tail_call(where, *arrays):
    rows, channels = arrays[1].shape
    block = arrays[-1].shape[1]
    return pl.pallas_call(
        tail_kernel,
        in_specs=[pl.BlockSpec(memory_space=pltpu.SMEM)] + held(len(arrays)),
        out_specs=pl.BlockSpec(memory_space=pltpu.VMEM),
        out_shape=jax.ShapeDtypeStruct((rows, channels), bf16),
        compiler_params=params(14),
        cost_estimate=pl.CostEstimate(
            flops=8 * rows * block * channels, bytes_accessed=7 << 20, transcendentals=0
        ),
        name="tail",
    )(where, *arrays)


def combine_kernel(lanes, mine_ref, other_ref, cot_ref, grad_ref, piece_ref):
    group, _, cut = piece_ref.shape
    for peer in range(group):
        for level in range(cut // lanes):
            column = (level * group + peer) * lanes
            cols = slice(column, column + lanes)
            total = mine_ref[:, cols].astype(f32) + other_ref[:, cols].astype(f32)
            total = (total + cot_ref[:, cols].astype(f32)).astype(bf16)
            grad_ref[:, cols] = total
            piece_ref[peer, :, level * lanes : (level + 1) * lanes] = total


def combine_call(mine, other, cotangent, group, lanes):
    rows, width = mine.shape
    return pl.pallas_call(
        functools.partial(combine_kernel, lanes),
        in_specs=held(3),
        out_specs=held(2),
        out_shape=[
            jax.ShapeDtypeStruct((rows, width), bf16),
            jax.ShapeDtypeStruct((group, rows, width // group), bf16),
        ],
        compiler_params=params(10),
        cost_estimate=pl.CostEstimate(flops=1 << 28, bytes_accessed=5 << 20, transcendentals=0),
        name="combine",
    )(mine, other, cotangent)


def product_kernel(mask, where_ref, grads_ref, *refs):
    group = grads_ref.shape[0]
    lanes = refs[-1].shape[0]
    inner = lax.rem(where_ref[0], group)
    level = (where_ref[0] // group) ^ mask
    cols = pl.ds(pl.multiple_of(level * lanes, lanes), lanes)
    total = rows_of(grads_ref[inner, :, cols], refs[0][...])
    for k in range(1, group):
        total = total + rows_of(grads_ref[inner ^ k, :, cols], refs[k][...])
    refs[-1][...] = total.astype(refs[-1].dtype)


def product_call(mask, kind, lanes, where, grads, mixers):
    group, rows, _ = grads.shape
    channels = mixers[0].shape[1]
    return pl.pallas_call(
        functools.partial(product_kernel, mask),
        in_specs=[pl.BlockSpec(memory_space=pltpu.SMEM)] + held(1 + group),
        out_specs=pl.BlockSpec(memory_space=pltpu.VMEM),
        out_shape=jax.ShapeDtypeStruct((lanes, channels), kind),
        compiler_params=params(14),
        cost_estimate=pl.CostEstimate(
            flops=2 * group * rows * lanes * channels, bytes_accessed=6 << 20, transcendentals=0
        ),
    )(where, grads, *mixers)


def on_device(
    moe_input,
    cotangent,
    expert_ids,
    route_weight,
    gate_proj,
    up_proj,
    down_proj,
    out_weight,
    recur_input,
    gate_input,
    states,
    conv_taps,
    decay_gate_w,
    input_gate_w,
    decay_rate,
    decay_extra,
):
    experts = lax.axis_size("sp")
    cores = lax.axis_size("tp")
    place = lax.axis_index("sp")
    core = lax.axis_index("tp")
    group = 8 if experts % 8 == 0 else experts
    outer = experts // group
    tok_rows, width = moe_input.shape
    channels = recur_input.shape[1]
    top_count = expert_ids.shape[1]
    capacity = max(2, 4 * tok_rows // experts)
    share = capacity // cores
    own_slots = experts * share

    flat_ids = expert_ids.reshape(-1)
    onehot = (flat_ids[:, None] == jnp.arange(experts, dtype=jnp.int32)[None, :]).astype(jnp.int32)
    slot_rank = jnp.sum((jnp.cumsum(onehot, axis=0) - onehot) * onehot, axis=1)
    pair_slots = (flat_ids * capacity + slot_rank).reshape(tok_rows, top_count)
    slot_iota = jnp.arange(own_slots, dtype=jnp.int32)
    slot_ids = (slot_iota // share) * capacity + core * share + slot_iota % share
    hits = slot_ids[:, None, None] == pair_slots[None, :, :]
    placing = jnp.any(hits, axis=2).astype(bf16)
    send_rows = times(placing, moe_input).astype(bf16).reshape(experts, share, width)
    late = (gate_input, states, recur_input, cotangent, route_weight)
    send_rows, late = lax.optimization_barrier((send_rows, late))
    gate_input, states, recur_input, cotangent_late, route_weight = late
    got_rows = lax.all_to_all(send_rows, "sp", split_axis=0, concat_axis=0, tiled=True)
    edge = jnp.concatenate([recur_input[-3:].astype(f32), states[-1:]], axis=0)
    edge = shifted(edge, "sp", 1)
    slot_weight = jnp.sum(jnp.where(hits, route_weight[None, :, :], 0.0), axis=(1, 2))
    send_grads = times(placing, cotangent_late) * slot_weight[:, None]
    send_grads = send_grads.astype(bf16).reshape(experts, share, width)

    gate_float = gate_input.astype(f32)
    gelu_value, gelu_back = jax.vjp(jax.nn.gelu, gate_float)
    slope = states * gelu_back(jnp.ones_like(gate_float))[0]
    mixer_out = (states * gelu_value).astype(bf16)
    half = group // 2
    mixers = {0: mixer_out}
    mixers[half] = swapped(mixer_out, "sp", half)
    send_grads, mixers[half], gelu_value, slope, edge, got_rows = lax.optimization_barrier(
        (send_grads, mixers[half], gelu_value, slope, edge, got_rows)
    )
    got_grads = lax.all_to_all(send_grads, "sp", split_axis=0, concat_axis=0, tiled=True)
    for k in range(1, half):
        mixers[k] = swapped(mixer_out, "sp", k)
    extended = jnp.concatenate([edge[:3], recur_input.astype(f32)], axis=0)
    prev_state = edge[3:]
    taps = conv_taps.astype(f32)
    conv = taps[0] * extended[0:tok_rows]
    for tap in range(1, 4):
        conv = conv + taps[tap] * extended[tap : tap + tok_rows]
    blocks, block_width = decay_gate_w.shape[:2]
    conv_low = conv.astype(bf16)

    def by_block(value, weights):
        parts = [
            times(value[:, b * block_width : (b + 1) * block_width], weights[b]) for b in range(blocks)
        ]
        return jnp.concatenate(parts, axis=1)

    recur_gate = jax.nn.sigmoid(by_block(conv_low, decay_gate_w))
    input_gate = jax.nn.sigmoid(by_block(conv_low, input_gate_w))
    first_row = (place * tok_rows + jnp.arange(tok_rows, dtype=jnp.int32) == 0)[:, None]
    log_decay = -decay_scale * recur_gate * decay_rate[None, :] + decay_extra
    decay_value = jnp.exp(log_decay)
    mult = jnp.where(first_row, 1.0, jnp.sqrt(-jnp.expm1(2.0 * log_decay)))
    prev_states = jnp.concatenate([prev_state, states[:-1]], axis=0)
    next_decay = jnp.concatenate([decay_value[1:], jnp.ones((1, channels), f32)], axis=0)
    to_log = prev_states * decay_value - jnp.where(
        first_row, 0.0, input_gate * conv * decay_value * decay_value / mult
    )
    to_decay = to_log * (-decay_scale * decay_rate[None, :]) * recur_gate * (1.0 - recur_gate)
    to_input = mult * conv * input_gate * (1.0 - input_gate)
    direct = mult * input_gate

    rows_here = got_rows.reshape(own_slots, width)
    rows_there = swapped(rows_here, "tp", 1)
    weight_gate = gate_proj[0]
    weight_up = up_proj[0]
    weight_down = down_proj[0]
    pres = tuple(
        (times(rows, weight_gate), times(rows, weight_up)) for rows in (rows_here, rows_there)
    )
    gates = (next_decay, decay_value[:1], to_decay, to_input, direct)
    got_grads, mixers, pres, rows_there, gates = lax.optimization_barrier(
        (got_grads, mixers, pres, rows_there, gates)
    )
    next_decay, first_decay, to_decay, to_input, direct = gates
    for k in range(1, half):
        mixers[k ^ half] = swapped(mixers[half], "sp", k)
    grads_here = got_grads.reshape(own_slots, width)
    grads_there = swapped(grads_here, "tp", 1)

    def expert(pre, grads_in):
        gate_pre, up_pre = pre
        sigmoid_gate = jax.nn.sigmoid(gate_pre)
        silu_gate = gate_pre * sigmoid_gate
        hidden = (silu_gate * up_pre).astype(bf16)
        hidden_grad = cols_of(grads_in, weight_down)
        gate_pre_grad = (
            hidden_grad * up_pre * sigmoid_gate * (1.0 + gate_pre * (1.0 - sigmoid_gate))
        ).astype(bf16)
        up_pre_grad = (hidden_grad * silu_gate).astype(bf16)
        return hidden, gate_pre_grad, up_pre_grad

    hidden_h, gate_h, up_h = expert(pres[0], grads_here)
    grads_there, hidden_h, gate_h, up_h = lax.optimization_barrier((grads_there, hidden_h, gate_h, up_h))
    hidden_t, gate_t, up_t = expert(pres[1], grads_there)
    partial_t = cols_of(gate_t, weight_gate) + cols_of(up_t, weight_up)
    from_there = swapped(partial_t.astype(bf16), "tp", 1)
    partial_h = cols_of(gate_h, weight_gate) + cols_of(up_h, weight_up)
    shared = (partial_h + from_there.astype(f32)).astype(bf16).reshape(experts, share, width)
    back = lax.all_to_all(shared, "sp", split_axis=0, concat_axis=0, tiled=True)
    head_coef = shifted(jnp.stack([to_decay[:8], to_input[:8], direct[:8]]), "sp", -1)
    down_grad = rows_of(hidden_h, grads_here) + rows_of(hidden_t, grads_there)
    gate_weight_grad = rows_of(rows_here, gate_h) + rows_of(rows_there, gate_t)
    up_weight_grad = rows_of(rows_here, up_h) + rows_of(rows_there, up_t)
    weight_grads = (gate_weight_grad.astype(bf16), up_weight_grad.astype(bf16), down_grad.astype(bf16))
    back, weight_grads, head_coef, mixers = lax.optimization_barrier(
        (back, weight_grads, head_coef, mixers)
    )

    mine_back = rows_of(placing, back.reshape(own_slots, width)).astype(bf16)
    other_back = swapped(mine_back, "tp", 1)
    out_rows = width // experts
    where = place[None].astype(jnp.int32)
    input_grad, pieces = combine_call(mine_back, other_back, cotangent, group, out_rows)

    groups = [[base + peer for peer in range(group)] for base in range(0, experts, group)]
    grads = lax.all_to_all(
        pieces, "sp", split_axis=0, concat_axis=0, tiled=True, axis_index_groups=groups
    )
    gate_grad, local, cumul, ends, head = mixer_call(
        input_grad, out_weight, gelu_value, slope, next_decay, first_decay, experts
    )
    head = shifted(head, "sp", -1)
    ends = lax.all_to_all(ends, "sp", split_axis=0, concat_axis=0, tiled=True)
    mixers = [mixers[k] for k in range(group)]
    if out_rows % 128 == 0:
        def block_for(mask, kind):
            return product_call(mask, kind, out_rows, where, grads, mixers)
    else:
        full = sum(
            rows_of(lax.dynamic_index_in_dim(grads, place % group ^ k, 0, False), mixers[k])
            for k in range(group)
        ).reshape(outer, out_rows, channels)

        def block_for(mask, kind):
            return lax.dynamic_index_in_dim(full, place // group ^ mask, 0, False).astype(kind)

    received = []
    for mask in range(1, outer):
        received.append(swapped(block_for(mask, bf16), "sp", mask * group))
    out_weight_grad = block_for(0, f32)
    for part in received:
        out_weight_grad = out_weight_grad + part.astype(f32)

    recur_grad = tail_call(
        where, ends, local, cumul, to_decay, to_input, direct,
        head, head_coef, conv_taps, decay_gate_w, input_gate_w,
    )
    return (
        weight_grads[0][None],
        weight_grads[1][None],
        weight_grads[2][None],
        out_weight_grad,
        input_grad,
        recur_grad,
        gate_grad,
    )


def solution(mesh):
    return jax.shard_map(
        on_device,
        mesh=mesh,
        in_specs=(
            P("sp", None),
            P("sp", None),
            P("sp", None),
            P("sp", None),
            P("sp", None, "tp"),
            P("sp", None, "tp"),
            P("sp", "tp", None),
            P(None, "tp"),
            P("sp", "tp"),
            P("sp", "tp"),
            P("sp", "tp"),
            P(None, "tp"),
            P("tp", None, None),
            P("tp", None, None),
            P("tp"),
            P("sp", "tp"),
        ),
        out_specs=(
            P("sp", None, "tp"),
            P("sp", None, "tp"),
            P("sp", "tp", None),
            P("sp", "tp"),
            P("sp", None),
            P("sp", "tp"),
            P("sp", "tp"),
        ),
        check_vma=False,
    )
```

```python
import functools

import jax
import jax.numpy as jnp
from jax import lax
from jax.experimental import pallas as pl
from jax.experimental.pallas import tpu as pltpu
from jax.sharding import PartitionSpec as P


decay_scale = 8.0
f32 = jnp.float32
bf16 = jnp.bfloat16


def dot(left, right, contract):
    return lax.dot_general(left, right, (contract, ((), ())), preferred_element_type=f32)


def rows_of(left, right):
    return dot(left, right, ((0,), (0,)))


def cols_of(left, right):
    return dot(left, right, ((1,), (1,)))


def times(left, right):
    return dot(left, right, ((1,), (0,)))


def shifted(value, axis, steps):
    count = lax.axis_size(axis)
    pairs = [(s, s + steps) for s in range(max(0, -steps), min(count, count - steps))]
    return lax.ppermute(value, axis, pairs)


def swapped(value, axis, mask):
    count = lax.axis_size(axis)
    return lax.ppermute(value, axis, [(s, s ^ mask) for s in range(count)])


def back_scan(decays, values):
    rows = values.shape[0]
    inner = lax.broadcasted_iota(jnp.int32, values.shape, 0) % 8
    step = 1
    while step < rows:
        if step < 8:
            keep = inner < 8 - step
            later_a = jnp.where(keep, pltpu.roll(decays, rows - step, 0), 1.0)
            later_b = jnp.where(keep, pltpu.roll(values, rows - step, 0), 0.0)
            values = values + decays * later_b
            decays = decays * later_a
            step *= 2
        else:
            break
    tiles = rows // 8
    decay_out = [None] * tiles
    value_out = [None] * tiles
    carry_a = jnp.ones_like(values[:1])
    carry_b = jnp.zeros_like(values[:1])
    for tile in reversed(range(tiles)):
        part_a = decays[tile * 8 : tile * 8 + 8]
        part_b = values[tile * 8 : tile * 8 + 8]
        value_out[tile] = part_b + part_a * carry_b
        decay_out[tile] = part_a * carry_a
        carry_b = value_out[tile][:1]
        carry_a = decay_out[tile][:1]
    return decay_out, value_out


def held(count):
    return [pl.BlockSpec(memory_space=pltpu.VMEM)] * count


def params(mib):
    return pltpu.CompilerParams(vmem_limit_bytes=mib << 20)


def mixer_kernel(grad_ref, weight_ref, gelu_ref, slope_ref, next_ref, first_ref,
                 gate_ref, local_ref, cumul_ref, ends_ref, head_ref):
    mixer = jnp.dot(grad_ref[...], weight_ref[...], preferred_element_type=f32)
    gate_ref[...] = (mixer * slope_ref[...]).astype(bf16)
    decays, values = back_scan(next_ref[...], mixer * gelu_ref[...])
    for tile in range(0, len(values), 2):
        rows = slice(tile * 8, tile * 8 + 16)
        cumul_ref[rows] = jnp.concatenate(decays[tile : tile + 2], axis=0).astype(bf16)
        local_ref[rows] = jnp.concatenate(values[tile : tile + 2], axis=0).astype(bf16)
    head_ref[0] = values[0]
    head_ref[1] = decays[0]
    first = first_ref[...]
    both = jnp.concatenate([first * decays[0][:1], first * values[0][:1]], axis=0)
    for peer in range(ends_ref.shape[0]):
        ends_ref[peer] = both


def mixer_call(input_grad, out_weight, gelu, slope, next_decay, first, peers):
    rows, width = input_grad.shape
    channels = out_weight.shape[1]
    block = 256
    wide = pl.BlockSpec((rows, block), lambda i: (0, i))
    return pl.pallas_call(
        mixer_kernel,
        grid=(channels // block,),
        in_specs=[
            pl.BlockSpec((rows, width), lambda i: (0, 0)),
            pl.BlockSpec((width, block), lambda i: (0, i)),
            wide, wide, wide,
            pl.BlockSpec((1, block), lambda i: (0, i)),
        ],
        out_specs=[
            wide, wide, wide,
            pl.BlockSpec((peers, 2, block), lambda i: (0, 0, i)),
            pl.BlockSpec((2, 8, block), lambda i: (0, 0, i)),
        ],
        out_shape=[
            jax.ShapeDtypeStruct((rows, channels), bf16),
            jax.ShapeDtypeStruct((rows, channels), bf16),
            jax.ShapeDtypeStruct((rows, channels), bf16),
            jax.ShapeDtypeStruct((peers, 2, channels), f32),
            jax.ShapeDtypeStruct((2, 8, channels), f32),
        ],
        cost_estimate=pl.CostEstimate(
            flops=2 * rows * width * channels, bytes_accessed=8 << 20, transcendentals=0
        ),
        name="mixer",
    )(input_grad, out_weight, gelu, slope, next_decay, first)


def tail_kernel(where_ref, ends_ref, local_ref, cumul_ref, to_decay_ref, to_input_ref, direct_ref,
                head_ref, head_coef_ref, taps_ref, decay_w_ref, input_w_ref, out_ref):
    mine = where_ref[0]
    count = ends_ref.shape[0]
    block = decay_w_ref.shape[1]
    rows = local_ref.shape[0]
    taps = taps_ref[...].astype(f32)

    carry = jnp.zeros_like(local_ref[:1])
    head_carry = carry
    for place in reversed(range(1, count)):
        ends = ends_ref[place]
        longer = ends[1:2] + ends[0:1] * carry
        head_carry = jnp.where(place > mine + 1, longer, head_carry)
        carry = jnp.where(place > mine, longer, carry)

    for index in range(decay_w_ref.shape[0]):
        cols = slice(index * block, (index + 1) * block)
        decay_w = decay_w_ref[index]

        def wide(ref):
            return ref[:, cols].astype(f32)

        input_w = input_w_ref[index]

        def conv_grad(carried, to_decay, to_input, direct):
            decay_pre = (carried * to_decay).astype(bf16)
            input_pre = (carried * to_input).astype(bf16)
            return carried * direct + cols_of(decay_pre, decay_w) + cols_of(input_pre, input_w)

        main = conv_grad(
            wide(local_ref) + wide(cumul_ref) * carry[:, cols],
            wide(to_decay_ref), wide(to_input_ref), wide(direct_ref),
        )
        halo = conv_grad(
            head_ref[0, :, cols] + head_ref[1, :, cols] * head_carry[:, cols],
            head_coef_ref[0, :, cols], head_coef_ref[1, :, cols], head_coef_ref[2, :, cols],
        )
        whole = jnp.concatenate([main, halo], axis=0)
        total = taps[0:1, cols] * pltpu.roll(whole, whole.shape[0] - 3, 0)
        for tap in range(1, 3):
            total = total + taps[tap : tap + 1, cols] * pltpu.roll(whole, whole.shape[0] - 3 + tap, 0)
        total = total + taps[3:4, cols] * whole
        out_ref[:, cols] = total[:rows].astype(bf16)


def tail_call(where, *arrays):
    ends, local, decay_w = arrays[0], arrays[1], arrays[-1]
    rows, channels = local.shape
    width = decay_w.shape[1]
    block = 2 * width
    wide = pl.BlockSpec((rows, block), lambda i, s: (0, i))
    gate = pl.BlockSpec((2, width, width), lambda i, s: (i, 0, 0))
    return pl.pallas_call(
        tail_kernel,
        grid_spec=pltpu.PrefetchScalarGridSpec(
            num_scalar_prefetch=1,
            grid=(channels // block,),
            in_specs=[
                pl.BlockSpec((ends.shape[0], 2, block), lambda i, s: (0, 0, i)),
                wide, wide, wide, wide, wide,
                pl.BlockSpec((2, 8, block), lambda i, s: (0, 0, i)),
                pl.BlockSpec((3, 8, block), lambda i, s: (0, 0, i)),
                pl.BlockSpec((4, block), lambda i, s: (0, i)),
                gate, gate,
            ],
            out_specs=wide,
        ),
        out_shape=jax.ShapeDtypeStruct((rows, channels), bf16),
        cost_estimate=pl.CostEstimate(
            flops=8 * rows * width * channels, bytes_accessed=7 << 20, transcendentals=0
        ),
        name="tail",
    )(where, *arrays)


def combine_kernel(lanes, mine_ref, other_ref, cot_ref, grad_ref, piece_ref):
    group, _, cut = piece_ref.shape
    for peer in range(group):
        for level in range(cut // lanes):
            column = (level * group + peer) * lanes
            cols = slice(column, column + lanes)
            total = mine_ref[:, cols].astype(f32) + other_ref[:, cols].astype(f32)
            total = (total + cot_ref[:, cols].astype(f32)).astype(bf16)
            grad_ref[:, cols] = total
            piece_ref[peer, :, level * lanes : (level + 1) * lanes] = total


def combine_call(mine, other, cotangent, group, lanes):
    rows, width = mine.shape
    return pl.pallas_call(
        functools.partial(combine_kernel, lanes),
        in_specs=held(3),
        out_specs=held(2),
        out_shape=[
            jax.ShapeDtypeStruct((rows, width), bf16),
            jax.ShapeDtypeStruct((group, rows, width // group), bf16),
        ],
        compiler_params=params(10),
        cost_estimate=pl.CostEstimate(flops=1 << 28, bytes_accessed=5 << 20, transcendentals=0),
        name="combine",
    )(mine, other, cotangent)


def product_kernel(where_ref, grads_ref, *refs):
    group, _, _ = grads_ref.shape
    sources, (send_ref, own_ref), (buffer, sems) = refs[:group], refs[group : group + 2], refs[group + 2 :]
    lanes, channels = own_ref.shape
    copies = [pltpu.make_async_copy(sources[k], buffer.at[k], sems.at[k]) for k in range(group)]
    for copy in copies:
        copy.start()
    inner = lax.rem(where_ref[0], group)
    level = where_ref[0] // group
    half = group // 2
    block = 512

    def partial(mask, cols, first):
        side = pl.ds(pl.multiple_of((level ^ mask) * lanes, lanes), lanes)
        total = None
        for k in range(first, first + half):
            part = rows_of(grads_ref[inner ^ k, :, side], buffer[k, :, cols])
            total = part if total is None else total + part
        return total

    for copy in copies[:half]:
        copy.wait()
    spans = [slice(start, start + block) for start in range(0, channels, block)]
    firsts = {(mask, n): partial(mask, cols, 0) for mask in (1, 0) for n, cols in enumerate(spans)}
    for copy in copies[half:]:
        copy.wait()
    for n, cols in enumerate(spans):
        send_ref[:, cols] = (firsts[1, n] + partial(1, cols, half)).astype(bf16)
        own_ref[:, cols] = firsts[0, n] + partial(0, cols, half)


def product_call(lanes, where, grads, mixers):
    group, rows, cut = grads.shape
    channels = mixers[0].shape[1]
    return pl.pallas_call(
        product_kernel,
        in_specs=[pl.BlockSpec(memory_space=pltpu.SMEM)]
        + held(1)
        + [pl.BlockSpec(memory_space=pl.ANY)] * group,
        out_specs=held(2),
        out_shape=[
            jax.ShapeDtypeStruct((lanes, channels), bf16),
            jax.ShapeDtypeStruct((lanes, channels), f32),
        ],
        scratch_shapes=[
            pltpu.VMEM((group, rows, channels), bf16),
            pltpu.SemaphoreType.DMA((group,)),
        ],
        compiler_params=params(24),
        cost_estimate=pl.CostEstimate(
            flops=2 * group * rows * cut * channels, bytes_accessed=6 << 20, transcendentals=0
        ),
        name="product",
    )(where, grads, *mixers)


def on_device(
    moe_input,
    cotangent,
    expert_ids,
    route_weight,
    gate_proj,
    up_proj,
    down_proj,
    out_weight,
    recur_input,
    gate_input,
    states,
    conv_taps,
    decay_gate_w,
    input_gate_w,
    decay_rate,
    decay_extra,
):
    experts = lax.axis_size("sp")
    cores = lax.axis_size("tp")
    place = lax.axis_index("sp")
    core = lax.axis_index("tp")
    group = 8 if experts % 8 == 0 else experts
    outer = experts // group
    tok_rows, width = moe_input.shape
    channels = recur_input.shape[1]
    top_count = expert_ids.shape[1]
    capacity = max(2, 4 * tok_rows // experts)
    share = capacity // cores
    own_slots = experts * share

    flat_ids = expert_ids.reshape(-1)
    onehot = (flat_ids[:, None] == jnp.arange(experts, dtype=jnp.int32)[None, :]).astype(jnp.int32)
    slot_rank = jnp.sum((jnp.cumsum(onehot, axis=0) - onehot) * onehot, axis=1)
    pair_slots = (flat_ids * capacity + slot_rank).reshape(tok_rows, top_count)
    slot_iota = jnp.arange(own_slots, dtype=jnp.int32)
    slot_ids = (slot_iota // share) * capacity + core * share + slot_iota % share
    hits = slot_ids[:, None, None] == pair_slots[None, :, :]
    placing = jnp.any(hits, axis=2).astype(bf16)
    send_rows = times(placing, moe_input).astype(bf16).reshape(experts, share, width)
    late = (gate_input, states, recur_input, cotangent, route_weight)
    send_rows, late = lax.optimization_barrier((send_rows, late))
    gate_input, states, recur_input, cotangent_late, route_weight = late
    got_rows = lax.all_to_all(send_rows, "sp", split_axis=0, concat_axis=0, tiled=True)
    edge = jnp.concatenate([recur_input[-3:].astype(f32), states[-1:]], axis=0)
    edge = shifted(edge, "sp", 1)
    slot_weight = jnp.sum(jnp.where(hits, route_weight[None, :, :], 0.0), axis=(1, 2))
    send_grads = times(placing, cotangent_late) * slot_weight[:, None]
    send_grads = send_grads.astype(bf16).reshape(experts, share, width)

    gate_float = gate_input.astype(f32)
    gelu_value, gelu_back = jax.vjp(jax.nn.gelu, gate_float)
    slope = states * gelu_back(jnp.ones_like(gate_float))[0]
    mixer_out = (states * gelu_value).astype(bf16)
    half = group // 2
    mixers = {0: mixer_out}
    mixers[half] = swapped(mixer_out, "sp", half)
    send_grads, gelu_value, slope, edge, got_rows = lax.optimization_barrier(
        (send_grads, gelu_value, slope, edge, got_rows)
    )
    got_grads = lax.all_to_all(send_grads, "sp", split_axis=0, concat_axis=0, tiled=True)
    for k in range(1, half):
        mixers[k] = swapped(mixer_out, "sp", k)
    extended = jnp.concatenate([edge[:3], recur_input.astype(f32)], axis=0)
    prev_state = edge[3:]
    taps = conv_taps.astype(f32)
    conv = taps[0] * extended[0:tok_rows]
    for tap in range(1, 4):
        conv = conv + taps[tap] * extended[tap : tap + tok_rows]
    blocks, block_width = decay_gate_w.shape[:2]
    conv_low = conv.astype(bf16)

    def by_block(value, weights):
        parts = [
            times(value[:, b * block_width : (b + 1) * block_width], weights[b]) for b in range(blocks)
        ]
        return jnp.concatenate(parts, axis=1)

    recur_gate = jax.nn.sigmoid(by_block(conv_low, decay_gate_w))
    input_gate = jax.nn.sigmoid(by_block(conv_low, input_gate_w))
    first_row = (place * tok_rows + jnp.arange(tok_rows, dtype=jnp.int32) == 0)[:, None]
    log_decay = -decay_scale * recur_gate * decay_rate[None, :] + decay_extra
    decay_value = jnp.exp(log_decay)
    mult = jnp.where(first_row, 1.0, jnp.sqrt(-jnp.expm1(2.0 * log_decay)))
    prev_states = jnp.concatenate([prev_state, states[:-1]], axis=0)
    next_decay = jnp.concatenate([decay_value[1:], jnp.ones((1, channels), f32)], axis=0)
    to_log = prev_states * decay_value - jnp.where(
        first_row, 0.0, input_gate * conv * decay_value * decay_value / mult
    )
    to_decay = to_log * (-decay_scale * decay_rate[None, :]) * recur_gate * (1.0 - recur_gate)
    to_input = mult * conv * input_gate * (1.0 - input_gate)
    direct = mult * input_gate

    rows_here = got_rows.reshape(own_slots, width)
    rows_there = swapped(rows_here, "tp", 1)
    weight_gate = gate_proj[0]
    weight_up = up_proj[0]
    weight_down = down_proj[0]
    pres = tuple(
        (times(rows, weight_gate), times(rows, weight_up)) for rows in (rows_here, rows_there)
    )
    head_coef = jnp.stack([to_decay[:8], to_input[:8], direct[:8]])
    gates = (
        next_decay, decay_value[:1], head_coef,
        to_decay.astype(bf16), to_input.astype(bf16), direct.astype(bf16),
    )
    got_grads, pres, rows_there, gates = lax.optimization_barrier((got_grads, pres, rows_there, gates))
    next_decay, first_decay, head_coef, to_decay, to_input, direct = gates
    for k in range(1, half):
        mixers[k ^ half] = swapped(mixers[half], "sp", k)
    grads_here = got_grads.reshape(own_slots, width)
    grads_there = swapped(grads_here, "tp", 1)

    def expert(pre, grads_in):
        gate_pre, up_pre = pre
        sigmoid_gate = jax.nn.sigmoid(gate_pre)
        silu_gate = gate_pre * sigmoid_gate
        hidden = (silu_gate * up_pre).astype(bf16)
        hidden_grad = cols_of(grads_in, weight_down)
        gate_pre_grad = (
            hidden_grad * up_pre * sigmoid_gate * (1.0 + gate_pre * (1.0 - sigmoid_gate))
        ).astype(bf16)
        up_pre_grad = (hidden_grad * silu_gate).astype(bf16)
        return hidden, gate_pre_grad, up_pre_grad

    hidden_h, gate_h, up_h = expert(pres[0], grads_here)
    grads_there, hidden_h, gate_h, up_h = lax.optimization_barrier((grads_there, hidden_h, gate_h, up_h))
    hidden_t, gate_t, up_t = expert(pres[1], grads_there)
    partial_t = cols_of(gate_t, weight_gate) + cols_of(up_t, weight_up)
    from_there = swapped(partial_t.astype(bf16), "tp", 1)
    partial_h = cols_of(gate_h, weight_gate) + cols_of(up_h, weight_up)
    shared = (partial_h + from_there.astype(f32)).astype(bf16).reshape(experts, share, width)
    back = lax.all_to_all(shared, "sp", split_axis=0, concat_axis=0, tiled=True)
    head_coef = shifted(head_coef, "sp", -1)
    down_grad = rows_of(hidden_h, grads_here) + rows_of(hidden_t, grads_there)
    gate_weight_grad = rows_of(rows_here, gate_h) + rows_of(rows_there, gate_t)
    up_weight_grad = rows_of(rows_here, up_h) + rows_of(rows_there, up_t)
    weight_grads = (gate_weight_grad.astype(bf16), up_weight_grad.astype(bf16), down_grad.astype(bf16))
    back, weight_grads, head_coef, mixers = lax.optimization_barrier(
        (back, weight_grads, head_coef, mixers)
    )

    mine_back = rows_of(placing, back.reshape(own_slots, width)).astype(bf16)
    other_back = swapped(mine_back, "tp", 1)
    out_rows = width // experts
    where = place[None].astype(jnp.int32)
    input_grad, pieces = combine_call(mine_back, other_back, cotangent, group, out_rows)

    groups = [[base + peer for peer in range(group)] for base in range(0, experts, group)]
    grads = lax.all_to_all(
        pieces, "sp", split_axis=0, concat_axis=0, tiled=True, axis_index_groups=groups
    )
    gate_grad, local, cumul, ends, head = mixer_call(
        input_grad, out_weight, gelu_value, slope, next_decay, first_decay, experts
    )
    head = shifted(head, "sp", -1)
    ends = lax.all_to_all(ends, "sp", split_axis=0, concat_axis=0, tiled=True)
    mixers = [mixers[k] for k in range(group)]
    received = []
    if outer == 2 and out_rows % 128 == 0:
        send, out_weight_grad = product_call(out_rows, where, grads, mixers)
        received.append(swapped(send, "sp", group))
    else:
        full = sum(
            rows_of(lax.dynamic_index_in_dim(grads, place % group ^ k, 0, False), mixers[k])
            for k in range(group)
        ).reshape(outer, out_rows, channels)

        def block_for(mask):
            return lax.dynamic_index_in_dim(full, place // group ^ mask, 0, False)

        for mask in range(1, outer):
            received.append(swapped(block_for(mask).astype(bf16), "sp", mask * group))
        out_weight_grad = block_for(0)
    for part in received:
        out_weight_grad = out_weight_grad + part.astype(f32)

    recur_grad = tail_call(
        where, ends, local, cumul, to_decay, to_input, direct,
        head, head_coef, conv_taps, decay_gate_w, input_gate_w,
    )
    return (
        weight_grads[0][None],
        weight_grads[1][None],
        weight_grads[2][None],
        out_weight_grad,
        input_grad,
        recur_grad,
        gate_grad,
    )


def solution(mesh):
    return jax.shard_map(
        on_device,
        mesh=mesh,
        in_specs=(
            P("sp", None),
            P("sp", None),
            P("sp", None),
            P("sp", None),
            P("sp", None, "tp"),
            P("sp", None, "tp"),
            P("sp", "tp", None),
            P(None, "tp"),
            P("sp", "tp"),
            P("sp", "tp"),
            P("sp", "tp"),
            P(None, "tp"),
            P("tp", None, None),
            P("tp", None, None),
            P("tp"),
            P("sp", "tp"),
        ),
        out_specs=(
            P("sp", None, "tp"),
            P("sp", None, "tp"),
            P("sp", "tp", None),
            P("sp", "tp"),
            P("sp", None),
            P("sp", "tp"),
            P("sp", "tp"),
        ),
        check_vma=False,
    )
```

```python
import functools

import jax
import jax.numpy as jnp
from jax import lax
from jax.experimental import pallas as pl
from jax.experimental.pallas import tpu as pltpu
from jax.sharding import PartitionSpec as P


decay_scale = 8.0
f32 = jnp.float32
bf16 = jnp.bfloat16


def dot(left, right, contract):
    return lax.dot_general(left, right, (contract, ((), ())), preferred_element_type=f32)


def rows_of(left, right):
    return dot(left, right, ((0,), (0,)))


def cols_of(left, right):
    return dot(left, right, ((1,), (1,)))


def times(left, right):
    return dot(left, right, ((1,), (0,)))


def shifted(value, axis, steps):
    count = lax.axis_size(axis)
    pairs = [(s, s + steps) for s in range(max(0, -steps), min(count, count - steps))]
    return lax.ppermute(value, axis, pairs)


def swapped(value, axis, mask):
    count = lax.axis_size(axis)
    return lax.ppermute(value, axis, [(s, s ^ mask) for s in range(count)])


def back_scan(decays, values):
    rows = values.shape[0]
    inner = lax.broadcasted_iota(jnp.int32, values.shape, 0) % 8
    step = 1
    while step < rows:
        if step < 8:
            keep = inner < 8 - step
            later_a = jnp.where(keep, pltpu.roll(decays, rows - step, 0), 1.0)
            later_b = jnp.where(keep, pltpu.roll(values, rows - step, 0), 0.0)
            values = values + decays * later_b
            decays = decays * later_a
            step *= 2
        else:
            break
    tiles = rows // 8
    decay_out = [None] * tiles
    value_out = [None] * tiles
    carry_a = jnp.ones_like(values[:1])
    carry_b = jnp.zeros_like(values[:1])
    for tile in reversed(range(tiles)):
        part_a = decays[tile * 8 : tile * 8 + 8]
        part_b = values[tile * 8 : tile * 8 + 8]
        value_out[tile] = part_b + part_a * carry_b
        decay_out[tile] = part_a * carry_a
        carry_b = value_out[tile][:1]
        carry_a = decay_out[tile][:1]
    return decay_out, value_out


def held(count):
    return [pl.BlockSpec(memory_space=pltpu.VMEM)] * count


def params(mib):
    return pltpu.CompilerParams(vmem_limit_bytes=mib << 20)


def mixer_kernel(grad_ref, weight_ref, gelu_ref, slope_ref, next_ref, first_ref,
                 gate_ref, local_ref, cumul_ref, ends_ref, head_ref):
    mixer = jnp.dot(grad_ref[...], weight_ref[...], preferred_element_type=f32)
    gate_ref[...] = (mixer * slope_ref[...]).astype(bf16)
    decays, values = back_scan(next_ref[...], mixer * gelu_ref[...])
    for tile in range(0, len(values), 2):
        rows = slice(tile * 8, tile * 8 + 16)
        cumul_ref[rows] = jnp.concatenate(decays[tile : tile + 2], axis=0).astype(bf16)
        local_ref[rows] = jnp.concatenate(values[tile : tile + 2], axis=0).astype(bf16)
    head_ref[0] = values[0]
    head_ref[1] = decays[0]
    first = first_ref[...]
    both = jnp.concatenate([first * decays[0][:1], first * values[0][:1]], axis=0)
    for peer in range(ends_ref.shape[0]):
        ends_ref[peer] = both


def mixer_call(input_grad, out_weight, gelu, slope, next_decay, first, peers):
    rows, width = input_grad.shape
    channels = out_weight.shape[1]
    block = 256
    wide = pl.BlockSpec((rows, block), lambda i: (0, i))
    return pl.pallas_call(
        mixer_kernel,
        grid=(channels // block,),
        in_specs=[
            pl.BlockSpec((rows, width), lambda i: (0, 0)),
            pl.BlockSpec((width, block), lambda i: (0, i)),
            wide, wide, wide,
            pl.BlockSpec((1, block), lambda i: (0, i)),
        ],
        out_specs=[
            wide, wide, wide,
            pl.BlockSpec((peers, 2, block), lambda i: (0, 0, i)),
            pl.BlockSpec((2, 8, block), lambda i: (0, 0, i)),
        ],
        out_shape=[
            jax.ShapeDtypeStruct((rows, channels), bf16),
            jax.ShapeDtypeStruct((rows, channels), bf16),
            jax.ShapeDtypeStruct((rows, channels), bf16),
            jax.ShapeDtypeStruct((peers, 2, channels), f32),
            jax.ShapeDtypeStruct((2, 8, channels), f32),
        ],
        cost_estimate=pl.CostEstimate(
            flops=2 * rows * width * channels, bytes_accessed=8 << 20, transcendentals=0
        ),
        name="mixer",
    )(input_grad, out_weight, gelu, slope, next_decay, first)


def tail_kernel(where_ref, ends_ref, local_ref, cumul_ref, to_decay_ref, to_input_ref, direct_ref,
                head_ref, head_coef_ref, taps_ref, decay_w_ref, input_w_ref, out_ref):
    mine = where_ref[0]
    count = ends_ref.shape[0]
    block = decay_w_ref.shape[1]
    rows = local_ref.shape[0]
    taps = taps_ref[...].astype(f32)

    carry = jnp.zeros_like(local_ref[:1])
    head_carry = carry
    for place in reversed(range(1, count)):
        ends = ends_ref[place]
        longer = ends[1:2] + ends[0:1] * carry
        head_carry = jnp.where(place > mine + 1, longer, head_carry)
        carry = jnp.where(place > mine, longer, carry)

    for index in range(decay_w_ref.shape[0]):
        cols = slice(index * block, (index + 1) * block)
        decay_w = decay_w_ref[index]

        def wide(ref):
            return ref[:, cols].astype(f32)

        input_w = input_w_ref[index]

        def conv_grad(carried, to_decay, to_input, direct):
            decay_pre = (carried * to_decay).astype(bf16)
            input_pre = (carried * to_input).astype(bf16)
            return carried * direct + cols_of(decay_pre, decay_w) + cols_of(input_pre, input_w)

        main = conv_grad(
            wide(local_ref) + wide(cumul_ref) * carry[:, cols],
            wide(to_decay_ref), wide(to_input_ref), wide(direct_ref),
        )
        halo = conv_grad(
            head_ref[0, :, cols] + head_ref[1, :, cols] * head_carry[:, cols],
            head_coef_ref[0, :, cols], head_coef_ref[1, :, cols], head_coef_ref[2, :, cols],
        )
        whole = jnp.concatenate([main, halo], axis=0)
        total = taps[0:1, cols] * pltpu.roll(whole, whole.shape[0] - 3, 0)
        for tap in range(1, 3):
            total = total + taps[tap : tap + 1, cols] * pltpu.roll(whole, whole.shape[0] - 3 + tap, 0)
        total = total + taps[3:4, cols] * whole
        out_ref[:, cols] = total[:rows].astype(bf16)


def tail_call(where, *arrays):
    ends, local, decay_w = arrays[0], arrays[1], arrays[-1]
    rows, channels = local.shape
    width = decay_w.shape[1]
    block = 2 * width
    wide = pl.BlockSpec((rows, block), lambda i, s: (0, i))
    gate = pl.BlockSpec((2, width, width), lambda i, s: (i, 0, 0))
    return pl.pallas_call(
        tail_kernel,
        grid_spec=pltpu.PrefetchScalarGridSpec(
            num_scalar_prefetch=1,
            grid=(channels // block,),
            in_specs=[
                pl.BlockSpec((ends.shape[0], 2, block), lambda i, s: (0, 0, i)),
                wide, wide, wide, wide, wide,
                pl.BlockSpec((2, 8, block), lambda i, s: (0, 0, i)),
                pl.BlockSpec((3, 8, block), lambda i, s: (0, 0, i)),
                pl.BlockSpec((4, block), lambda i, s: (0, i)),
                gate, gate,
            ],
            out_specs=wide,
        ),
        out_shape=jax.ShapeDtypeStruct((rows, channels), bf16),
        cost_estimate=pl.CostEstimate(
            flops=8 * rows * width * channels, bytes_accessed=7 << 20, transcendentals=0
        ),
        name="tail",
    )(where, *arrays)


def combine_kernel(lanes, mine_ref, other_ref, cot_ref, grad_ref, piece_ref):
    group, _, cut = piece_ref.shape
    for peer in range(group):
        for level in range(cut // lanes):
            column = (level * group + peer) * lanes
            cols = slice(column, column + lanes)
            total = mine_ref[:, cols].astype(f32) + other_ref[:, cols].astype(f32)
            total = (total + cot_ref[:, cols].astype(f32)).astype(bf16)
            grad_ref[:, cols] = total
            piece_ref[peer, :, level * lanes : (level + 1) * lanes] = total


def combine_call(mine, other, cotangent, group, lanes):
    rows, width = mine.shape
    return pl.pallas_call(
        functools.partial(combine_kernel, lanes),
        in_specs=held(3),
        out_specs=held(2),
        out_shape=[
            jax.ShapeDtypeStruct((rows, width), bf16),
            jax.ShapeDtypeStruct((group, rows, width // group), bf16),
        ],
        compiler_params=params(10),
        cost_estimate=pl.CostEstimate(flops=1 << 28, bytes_accessed=5 << 20, transcendentals=0),
        name="combine",
    )(mine, other, cotangent)


def product_kernel(where_ref, grads_ref, *refs):
    group, _, _ = grads_ref.shape
    sources, (send_ref, own_ref), (buffer, sems) = refs[:group], refs[group : group + 2], refs[group + 2 :]
    lanes, channels = own_ref.shape
    copies = [pltpu.make_async_copy(sources[k], buffer.at[k], sems.at[k]) for k in range(group)]
    for copy in copies:
        copy.start()
    inner = lax.rem(where_ref[0], group)
    level = where_ref[0] // group
    half = group // 2
    block = 512

    def partial(mask, cols, first):
        side = pl.ds(pl.multiple_of((level ^ mask) * lanes, lanes), lanes)
        total = None
        for k in range(first, first + half):
            part = rows_of(grads_ref[inner ^ k, :, side], buffer[k, :, cols])
            total = part if total is None else total + part
        return total

    for copy in copies[:half]:
        copy.wait()
    spans = [slice(start, start + block) for start in range(0, channels, block)]
    firsts = {(mask, n): partial(mask, cols, 0) for mask in (1, 0) for n, cols in enumerate(spans)}
    for copy in copies[half:]:
        copy.wait()
    for n, cols in enumerate(spans):
        send_ref[:, cols] = (firsts[1, n] + partial(1, cols, half)).astype(bf16)
        own_ref[:, cols] = firsts[0, n] + partial(0, cols, half)


def product_call(lanes, where, grads, mixers):
    group, rows, cut = grads.shape
    channels = mixers[0].shape[1]
    return pl.pallas_call(
        product_kernel,
        in_specs=[pl.BlockSpec(memory_space=pltpu.SMEM)]
        + held(1)
        + [pl.BlockSpec(memory_space=pl.ANY)] * group,
        out_specs=held(2),
        out_shape=[
            jax.ShapeDtypeStruct((lanes, channels), bf16),
            jax.ShapeDtypeStruct((lanes, channels), f32),
        ],
        scratch_shapes=[
            pltpu.VMEM((group, rows, channels), bf16),
            pltpu.SemaphoreType.DMA((group,)),
        ],
        compiler_params=params(24),
        cost_estimate=pl.CostEstimate(
            flops=2 * group * rows * cut * channels, bytes_accessed=6 << 20, transcendentals=0
        ),
        name="product",
    )(where, grads, *mixers)


def on_device(
    moe_input,
    cotangent,
    expert_ids,
    route_weight,
    gate_proj,
    up_proj,
    down_proj,
    out_weight,
    recur_input,
    gate_input,
    states,
    conv_taps,
    decay_gate_w,
    input_gate_w,
    decay_rate,
    decay_extra,
):
    experts = lax.axis_size("sp")
    cores = lax.axis_size("tp")
    place = lax.axis_index("sp")
    core = lax.axis_index("tp")
    group = 8 if experts % 8 == 0 else experts
    outer = experts // group
    tok_rows, width = moe_input.shape
    channels = recur_input.shape[1]
    top_count = expert_ids.shape[1]
    capacity = max(2, 4 * tok_rows // experts)
    share = capacity // cores
    own_slots = experts * share

    flat_ids = expert_ids.reshape(-1)
    onehot = (flat_ids[:, None] == jnp.arange(experts, dtype=jnp.int32)[None, :]).astype(jnp.int32)
    slot_rank = jnp.sum((jnp.cumsum(onehot, axis=0) - onehot) * onehot, axis=1)
    pair_slots = (flat_ids * capacity + slot_rank).reshape(tok_rows, top_count)
    slot_iota = jnp.arange(own_slots, dtype=jnp.int32)
    slot_ids = (slot_iota // share) * capacity + core * share + slot_iota % share
    hits = slot_ids[:, None, None] == pair_slots[None, :, :]
    placing = jnp.any(hits, axis=2).astype(bf16)
    send_rows = times(placing, moe_input).astype(bf16).reshape(experts, share, width)
    late = (gate_input, states, recur_input, cotangent, route_weight)
    send_rows, late = lax.optimization_barrier((send_rows, late))
    gate_input, states, recur_input, cotangent_late, route_weight = late
    got_rows = lax.all_to_all(send_rows, "sp", split_axis=0, concat_axis=0, tiled=True)
    own_weights = (gate_proj[0], up_proj[0], down_proj[0])
    other_weights = tuple(swapped(weight, "tp", 1) for weight in own_weights)
    edge = jnp.concatenate([recur_input[-3:].astype(f32), states[-1:]], axis=0)
    edge = shifted(edge, "sp", 1)
    slot_weight = jnp.sum(jnp.where(hits, route_weight[None, :, :], 0.0), axis=(1, 2))
    send_grads = times(placing, cotangent_late) * slot_weight[:, None]
    send_grads = send_grads.astype(bf16).reshape(experts, share, width)

    gate_float = gate_input.astype(f32)
    gelu_value, gelu_back = jax.vjp(jax.nn.gelu, gate_float)
    slope = states * gelu_back(jnp.ones_like(gate_float))[0]
    mixer_out = (states * gelu_value).astype(bf16)
    half = group // 2
    mixers = {0: mixer_out}
    mixers[half] = swapped(mixer_out, "sp", half)
    send_grads, gelu_value, slope, edge, got_rows = lax.optimization_barrier(
        (send_grads, gelu_value, slope, edge, got_rows)
    )
    got_grads = lax.all_to_all(send_grads, "sp", split_axis=0, concat_axis=0, tiled=True)
    for k in range(1, half):
        mixers[k] = swapped(mixer_out, "sp", k)
    extended = jnp.concatenate([edge[:3], recur_input.astype(f32)], axis=0)
    prev_state = edge[3:]
    taps = conv_taps.astype(f32)
    conv = taps[0] * extended[0:tok_rows]
    for tap in range(1, 4):
        conv = conv + taps[tap] * extended[tap : tap + tok_rows]
    blocks, block_width = decay_gate_w.shape[:2]
    conv_low = conv.astype(bf16)

    def by_block(value, weights):
        parts = [
            times(value[:, b * block_width : (b + 1) * block_width], weights[b]) for b in range(blocks)
        ]
        return jnp.concatenate(parts, axis=1)

    recur_gate = jax.nn.sigmoid(by_block(conv_low, decay_gate_w))
    input_gate = jax.nn.sigmoid(by_block(conv_low, input_gate_w))
    first_row = (place * tok_rows + jnp.arange(tok_rows, dtype=jnp.int32) == 0)[:, None]
    log_decay = -decay_scale * recur_gate * decay_rate[None, :] + decay_extra
    decay_value = jnp.exp(log_decay)
    mult = jnp.where(first_row, 1.0, jnp.sqrt(-jnp.expm1(2.0 * log_decay)))
    prev_states = jnp.concatenate([prev_state, states[:-1]], axis=0)
    next_decay = jnp.concatenate([decay_value[1:], jnp.ones((1, channels), f32)], axis=0)
    to_log = prev_states * decay_value - jnp.where(
        first_row, 0.0, input_gate * conv * decay_value * decay_value / mult
    )
    to_decay = to_log * (-decay_scale * decay_rate[None, :]) * recur_gate * (1.0 - recur_gate)
    to_input = mult * conv * input_gate * (1.0 - input_gate)
    direct = mult * input_gate

    rows_here = got_rows.reshape(own_slots, width)
    rows_there = swapped(rows_here, "tp", 1)
    rows_here, rows_there = lax.optimization_barrier((rows_here, rows_there))

    def first_half(gate_w, up_w):
        gate_pre = times(rows_here, gate_w)
        up_pre = times(rows_here, up_w)
        sigmoid_gate = jax.nn.sigmoid(gate_pre)
        silu_gate = gate_pre * sigmoid_gate
        slope_gate = up_pre * sigmoid_gate * (1.0 + gate_pre * (1.0 - sigmoid_gate))
        return (silu_gate * up_pre).astype(bf16), silu_gate.astype(bf16), slope_gate.astype(bf16)

    pres = tuple(first_half(weights[0], weights[1]) for weights in (own_weights, other_weights))
    head_coef = jnp.stack([to_decay[:8], to_input[:8], direct[:8]])
    gates = (
        next_decay, decay_value[:1], head_coef,
        to_decay.astype(bf16), to_input.astype(bf16), direct.astype(bf16),
    )
    got_grads, pres, gates = lax.optimization_barrier((got_grads, pres, gates))
    next_decay, first_decay, head_coef, to_decay, to_input, direct = gates
    for k in range(1, half):
        mixers[k ^ half] = swapped(mixers[half], "sp", k)
    grads_here = got_grads.reshape(own_slots, width)

    def second_half(pre, down_w):
        hidden_grad = cols_of(grads_here, down_w)
        return (hidden_grad * pre[2].astype(f32)).astype(bf16), (hidden_grad * pre[1].astype(f32)).astype(bf16)

    own_grads = second_half(pres[0], own_weights[2])
    other_grads = second_half(pres[1], other_weights[2])
    partial = (
        cols_of(own_grads[0], own_weights[0])
        + cols_of(own_grads[1], own_weights[1])
        + cols_of(other_grads[0], other_weights[0])
        + cols_of(other_grads[1], other_weights[1])
    )
    shared = partial.astype(bf16).reshape(experts, share, width)
    back = lax.all_to_all(shared, "sp", split_axis=0, concat_axis=0, tiled=True)
    head_coef = shifted(head_coef, "sp", -1)
    hidden_h, gate_h, up_h = pres[0][0], own_grads[0], own_grads[1]
    grads_there = swapped(grads_here, "tp", 1)
    hidden_t = swapped(pres[1][0], "tp", 1)
    gate_t = swapped(other_grads[0], "tp", 1)
    up_t = swapped(other_grads[1], "tp", 1)
    down_grad = rows_of(hidden_h, grads_here) + rows_of(hidden_t, grads_there)
    gate_weight_grad = rows_of(rows_here, gate_h) + rows_of(rows_there, gate_t)
    up_weight_grad = rows_of(rows_here, up_h) + rows_of(rows_there, up_t)
    weight_grads = (gate_weight_grad.astype(bf16), up_weight_grad.astype(bf16), down_grad.astype(bf16))
    back, weight_grads, head_coef, mixers = lax.optimization_barrier(
        (back, weight_grads, head_coef, mixers)
    )

    mine_back = rows_of(placing, back.reshape(own_slots, width)).astype(bf16)
    other_back = swapped(mine_back, "tp", 1)
    out_rows = width // experts
    where = place[None].astype(jnp.int32)
    input_grad, pieces = combine_call(mine_back, other_back, cotangent, group, out_rows)

    groups = [[base + peer for peer in range(group)] for base in range(0, experts, group)]
    grads = lax.all_to_all(
        pieces, "sp", split_axis=0, concat_axis=0, tiled=True, axis_index_groups=groups
    )
    gate_grad, local, cumul, ends, head = mixer_call(
        input_grad, out_weight, gelu_value, slope, next_decay, first_decay, experts
    )
    head = shifted(head, "sp", -1)
    ends = lax.all_to_all(ends, "sp", split_axis=0, concat_axis=0, tiled=True)
    mixers = [mixers[k] for k in range(group)]
    received = []
    if outer == 2 and out_rows % 128 == 0:
        send, out_weight_grad = product_call(out_rows, where, grads, mixers)
        received.append(swapped(send, "sp", group))
    else:
        full = sum(
            rows_of(lax.dynamic_index_in_dim(grads, place % group ^ k, 0, False), mixers[k])
            for k in range(group)
        ).reshape(outer, out_rows, channels)

        def block_for(mask):
            return lax.dynamic_index_in_dim(full, place // group ^ mask, 0, False)

        for mask in range(1, outer):
            received.append(swapped(block_for(mask).astype(bf16), "sp", mask * group))
        out_weight_grad = block_for(0)
    for part in received:
        out_weight_grad = out_weight_grad + part.astype(f32)

    recur_grad = tail_call(
        where, ends, local, cumul, to_decay, to_input, direct,
        head, head_coef, conv_taps, decay_gate_w, input_gate_w,
    )
    return (
        weight_grads[0][None],
        weight_grads[1][None],
        weight_grads[2][None],
        out_weight_grad,
        input_grad,
        recur_grad,
        gate_grad,
    )


def solution(mesh):
    return jax.shard_map(
        on_device,
        mesh=mesh,
        in_specs=(
            P("sp", None),
            P("sp", None),
            P("sp", None),
            P("sp", None),
            P("sp", None, "tp"),
            P("sp", None, "tp"),
            P("sp", "tp", None),
            P(None, "tp"),
            P("sp", "tp"),
            P("sp", "tp"),
            P("sp", "tp"),
            P(None, "tp"),
            P("tp", None, None),
            P("tp", None, None),
            P("tp"),
            P("sp", "tp"),
        ),
        out_specs=(
            P("sp", None, "tp"),
            P("sp", None, "tp"),
            P("sp", "tp", None),
            P("sp", "tp"),
            P("sp", None),
            P("sp", "tp"),
            P("sp", "tp"),
        ),
        check_vma=False,
    )
```

```python
import functools

import jax
import jax.numpy as jnp
from jax import lax
from jax.experimental import pallas as pl
from jax.experimental.pallas import tpu as pltpu
from jax.sharding import PartitionSpec as P


decay_scale = 8.0
f32 = jnp.float32
bf16 = jnp.bfloat16


def dot(left, right, contract):
    return lax.dot_general(left, right, (contract, ((), ())), preferred_element_type=f32)


def rows_of(left, right):
    return dot(left, right, ((0,), (0,)))


def cols_of(left, right):
    return dot(left, right, ((1,), (1,)))


def times(left, right):
    return dot(left, right, ((1,), (0,)))


def shifted(value, axis, steps):
    count = lax.axis_size(axis)
    pairs = [(s, s + steps) for s in range(max(0, -steps), min(count, count - steps))]
    return lax.ppermute(value, axis, pairs)


def swapped(value, axis, mask):
    count = lax.axis_size(axis)
    return lax.ppermute(value, axis, [(s, s ^ mask) for s in range(count)])


def back_scan(decays, values):
    rows = values.shape[0]
    inner = lax.broadcasted_iota(jnp.int32, values.shape, 0) % 8
    step = 1
    while step < rows:
        if step < 8:
            keep = inner < 8 - step
            later_a = jnp.where(keep, pltpu.roll(decays, rows - step, 0), 1.0)
            later_b = jnp.where(keep, pltpu.roll(values, rows - step, 0), 0.0)
            values = values + decays * later_b
            decays = decays * later_a
            step *= 2
        else:
            break
    tiles = rows // 8
    decay_out = [None] * tiles
    value_out = [None] * tiles
    carry_a = jnp.ones_like(values[:1])
    carry_b = jnp.zeros_like(values[:1])
    for tile in reversed(range(tiles)):
        part_a = decays[tile * 8 : tile * 8 + 8]
        part_b = values[tile * 8 : tile * 8 + 8]
        value_out[tile] = part_b + part_a * carry_b
        decay_out[tile] = part_a * carry_a
        carry_b = value_out[tile][:1]
        carry_a = decay_out[tile][:1]
    return decay_out, value_out


def held(count):
    return [pl.BlockSpec(memory_space=pltpu.VMEM)] * count


def params(mib):
    return pltpu.CompilerParams(vmem_limit_bytes=mib << 20)


def mixer_kernel(grad_ref, weight_ref, gelu_ref, slope_ref, next_ref, first_ref,
                 gate_ref, local_ref, cumul_ref, ends_ref, head_ref):
    mixer = jnp.dot(grad_ref[...], weight_ref[...], preferred_element_type=f32)
    gate_ref[...] = (mixer * slope_ref[...]).astype(bf16)
    decays, values = back_scan(next_ref[...], mixer * gelu_ref[...])
    for tile in range(0, len(values), 2):
        rows = slice(tile * 8, tile * 8 + 16)
        cumul_ref[rows] = jnp.concatenate(decays[tile : tile + 2], axis=0).astype(bf16)
        local_ref[rows] = jnp.concatenate(values[tile : tile + 2], axis=0).astype(bf16)
    head_ref[0] = values[0]
    head_ref[1] = decays[0]
    first = first_ref[...]
    ends_ref[...] = jnp.concatenate([first * decays[0][:1], first * values[0][:1]], axis=0)


def mixer_call(input_grad, out_weight, gelu, slope, next_decay, first):
    rows, width = input_grad.shape
    channels = out_weight.shape[1]
    block = 256
    wide = pl.BlockSpec((rows, block), lambda i: (0, i))
    return pl.pallas_call(
        mixer_kernel,
        grid=(channels // block,),
        in_specs=[
            pl.BlockSpec((rows, width), lambda i: (0, 0)),
            pl.BlockSpec((width, block), lambda i: (0, i)),
            wide, wide, wide,
            pl.BlockSpec((1, block), lambda i: (0, i)),
        ],
        out_specs=[
            wide, wide, wide,
            pl.BlockSpec((2, block), lambda i: (0, i)),
            pl.BlockSpec((2, 8, block), lambda i: (0, 0, i)),
        ],
        out_shape=[
            jax.ShapeDtypeStruct((rows, channels), bf16),
            jax.ShapeDtypeStruct((rows, channels), bf16),
            jax.ShapeDtypeStruct((rows, channels), bf16),
            jax.ShapeDtypeStruct((2, channels), f32),
            jax.ShapeDtypeStruct((2, 8, channels), f32),
        ],
        cost_estimate=pl.CostEstimate(
            flops=2 * rows * width * channels, bytes_accessed=8 << 20, transcendentals=0
        ),
        name="mixer",
    )(input_grad, out_weight, gelu, slope, next_decay, first)


def joined(near, far_a, far_b):
    return near[0:1] * far_a, near[1:2] + near[0:1] * far_b


def chosen(refs, wanted):
    value = refs[0][...]
    for k in range(1, len(refs)):
        value = jnp.where(wanted == k, refs[k][...], value)
    return value


def near_kernel(where_ref, *refs):
    later_ref, total_ref = refs[-2:]
    ends = refs[:-2]
    count = len(ends)
    mine = lax.rem(where_ref[0], count)
    whole = (jnp.ones_like(ends[0][:1]), jnp.zeros_like(ends[0][:1]))
    later = whole
    for spot in reversed(range(count)):
        whole = joined(chosen(ends, mine ^ spot), *whole)
        later = tuple(jnp.where(spot > mine, new, old) for new, old in zip(whole, later))
    later_ref[...] = jnp.concatenate(later, axis=0)
    total_ref[...] = jnp.concatenate(whole, axis=0)


def near_call(where, ends):
    shape = jax.ShapeDtypeStruct(ends[0].shape, f32)
    return pl.pallas_call(
        near_kernel,
        in_specs=[pl.BlockSpec(memory_space=pltpu.SMEM)] + held(len(ends)),
        out_specs=held(2),
        out_shape=[shape, shape],
        compiler_params=params(4),
        cost_estimate=pl.CostEstimate(flops=1 << 20, bytes_accessed=1 << 16, transcendentals=0),
        name="near",
    )(where, *ends)


def tail_kernel(count, where_ref, later_ref, next_ref, *refs):
    far = refs[:count]
    (local_ref, cumul_ref, to_decay_ref, to_input_ref, direct_ref,
     head_ref, head_coef_ref, taps_ref, decay_w_ref, input_w_ref, out_ref) = refs[count:]
    near = where_ref[1]
    mine = where_ref[0] // near
    after = (where_ref[0] + 1) // near
    block = decay_w_ref.shape[1]
    rows = local_ref.shape[0]
    taps = taps_ref[...].astype(f32)

    carry = jnp.zeros_like(later_ref[:1])
    head_carry = carry
    for spot in reversed(range(1, count)):
        total = chosen(far, mine ^ spot)
        longer = total[1:2] + total[0:1] * carry
        head_carry = jnp.where(spot > after, longer, head_carry)
        carry = jnp.where(spot > mine, longer, carry)
    carry = later_ref[1:2] + later_ref[0:1] * carry
    head_carry = next_ref[1:2] + next_ref[0:1] * head_carry

    for index in range(decay_w_ref.shape[0]):
        cols = slice(index * block, (index + 1) * block)
        decay_w = decay_w_ref[index]

        def wide(ref):
            return ref[:, cols].astype(f32)

        input_w = input_w_ref[index]

        def conv_grad(carried, to_decay, to_input, direct):
            decay_pre = (carried * to_decay).astype(bf16)
            input_pre = (carried * to_input).astype(bf16)
            return carried * direct + cols_of(decay_pre, decay_w) + cols_of(input_pre, input_w)

        main = conv_grad(
            wide(local_ref) + wide(cumul_ref) * carry[:, cols],
            wide(to_decay_ref), wide(to_input_ref), wide(direct_ref),
        )
        halo = conv_grad(
            head_ref[0, :, cols] + head_ref[1, :, cols] * head_carry[:, cols],
            head_coef_ref[0, :, cols], head_coef_ref[1, :, cols], head_coef_ref[2, :, cols],
        )
        whole = jnp.concatenate([main, halo], axis=0)
        total = taps[0:1, cols] * pltpu.roll(whole, whole.shape[0] - 3, 0)
        for tap in range(1, 3):
            total = total + taps[tap : tap + 1, cols] * pltpu.roll(whole, whole.shape[0] - 3 + tap, 0)
        total = total + taps[3:4, cols] * whole
        out_ref[:, cols] = total[:rows].astype(bf16)


def tail_call(where, later, later_next, far, *arrays):
    local, decay_w = arrays[0], arrays[-1]
    rows, channels = local.shape
    width = decay_w.shape[1]
    block = 2 * width
    wide = pl.BlockSpec((rows, block), lambda i, s: (0, i))
    gate = pl.BlockSpec((2, width, width), lambda i, s: (i, 0, 0))
    pair = pl.BlockSpec((2, block), lambda i, s: (0, i))
    return pl.pallas_call(
        functools.partial(tail_kernel, len(far)),
        grid_spec=pltpu.PrefetchScalarGridSpec(
            num_scalar_prefetch=1,
            grid=(channels // block,),
            in_specs=[pair] * (2 + len(far)) + [
                wide, wide, wide, wide, wide,
                pl.BlockSpec((2, 8, block), lambda i, s: (0, 0, i)),
                pl.BlockSpec((3, 8, block), lambda i, s: (0, 0, i)),
                pl.BlockSpec((4, block), lambda i, s: (0, i)),
                gate, gate,
            ],
            out_specs=wide,
        ),
        out_shape=jax.ShapeDtypeStruct((rows, channels), bf16),
        cost_estimate=pl.CostEstimate(
            flops=8 * rows * width * channels, bytes_accessed=7 << 20, transcendentals=0
        ),
        name="tail",
    )(where, later, later_next, *far, *arrays)


def combine_kernel(lanes, mine_ref, other_ref, cot_ref, grad_ref, piece_ref):
    group, _, cut = piece_ref.shape
    for peer in range(group):
        for level in range(cut // lanes):
            column = (level * group + peer) * lanes
            cols = slice(column, column + lanes)
            total = mine_ref[:, cols].astype(f32) + other_ref[:, cols].astype(f32)
            total = (total + cot_ref[:, cols].astype(f32)).astype(bf16)
            grad_ref[:, cols] = total
            piece_ref[peer, :, level * lanes : (level + 1) * lanes] = total


def combine_call(mine, other, cotangent, group, lanes):
    rows, width = mine.shape
    return pl.pallas_call(
        functools.partial(combine_kernel, lanes),
        in_specs=held(3),
        out_specs=held(2),
        out_shape=[
            jax.ShapeDtypeStruct((rows, width), bf16),
            jax.ShapeDtypeStruct((group, rows, width // group), bf16),
        ],
        compiler_params=params(10),
        cost_estimate=pl.CostEstimate(flops=1 << 28, bytes_accessed=5 << 20, transcendentals=0),
        name="combine",
    )(mine, other, cotangent)


def expert_kernel(span, grads_ref, *refs):
    silus, slopes, downs, gates, ups = (refs[2 * n : 2 * n + 2] for n in range(5))
    out_ref, gate_outs, up_outs = refs[10], refs[11:13], refs[13:15]
    grads_v, pre_v, down_v, wide_v, out_v, sems = refs[15:]
    hidden, width = downs[0].shape
    used = []

    def fetch(source, target):
        copy = pltpu.make_async_copy(source, target, sems.at[len(used)])
        copy.start()
        used.append(copy)
        return copy

    chunks = [(side, start) for side in range(2) for start in range(0, hidden, span)]
    grads_copy = fetch(grads_ref, grads_v)
    chunk_copies = {}
    for side, start in chunks:
        rows = pl.ds(start, span)
        chunk_copies[side, start] = [fetch(downs[side].at[rows], down_v.at[side, rows])]
        if start == 0:
            chunk_copies[side, start] += [
                fetch(silus[side], pre_v.at[side]), fetch(slopes[side], pre_v.at[2 + side])
            ]
    blocks = range(0, width, span)
    wide_copies = {
        start: [
            fetch(source.at[pl.ds(start, span)], wide_v.at[n, pl.ds(start, span)])
            for n, source in enumerate((*gates, *ups))
        ]
        for start in blocks
    }
    grads_copy.wait()
    for side, start in chunks:
        for copy in chunk_copies[side, start]:
            copy.wait()
        cols = slice(start, start + span)
        hidden_grad = cols_of(grads_v[...], down_v[side, cols, :])
        gate_outs[side][:, cols] = (hidden_grad * pre_v[2 + side, :, cols].astype(f32)).astype(bf16)
        up_outs[side][:, cols] = (hidden_grad * pre_v[side, :, cols].astype(f32)).astype(bf16)
    results = []
    for start in blocks:
        for copy in wide_copies[start]:
            copy.wait()
        cols = slice(start, start + span)
        total = None
        for n, part_ref in enumerate((*gate_outs, *up_outs)):
            part = cols_of(part_ref[...], wide_v[n, cols, :])
            total = part if total is None else total + part
        out_v[:, cols] = total.astype(bf16)
        results.append(fetch(out_v.at[:, pl.ds(start, span)], out_ref.at[:, pl.ds(start, span)]))
    for copy in results:
        copy.wait()


def expert_call(grads, pres, weights):
    slots, width = grads.shape
    hidden = weights[0][2].shape[0]
    span = min(256, hidden)
    arrays = [pre[1] for pre in pres] + [pre[2] for pre in pres]
    for n in (2, 0, 1):
        arrays += [weight[n] for weight in weights]
    part = jax.ShapeDtypeStruct((slots, hidden), bf16)
    count = 1 + 2 * (hidden // span) + 4 + 5 * (width // span)
    return pl.pallas_call(
        functools.partial(expert_kernel, span),
        in_specs=[pl.BlockSpec(memory_space=pl.ANY)] * (1 + len(arrays)),
        out_specs=[pl.BlockSpec(memory_space=pl.ANY)] + held(4),
        out_shape=[jax.ShapeDtypeStruct((slots, width), bf16)] + [part] * 4,
        scratch_shapes=[
            pltpu.VMEM((slots, width), bf16),
            pltpu.VMEM((4, slots, hidden), bf16),
            pltpu.VMEM((2, hidden, width), bf16),
            pltpu.VMEM((4, width, hidden), bf16),
            pltpu.VMEM((slots, width), bf16),
            pltpu.SemaphoreType.DMA((count,)),
        ],
        compiler_params=params(36),
        cost_estimate=pl.CostEstimate(
            flops=12 * slots * width * hidden, bytes_accessed=18 << 20, transcendentals=0
        ),
        name="expert",
    )(grads, *arrays)


def product_kernel(where_ref, grads_ref, *refs):
    group, _, _ = grads_ref.shape
    sources, (send_ref, own_ref), (buffer, sems) = refs[:group], refs[group : group + 2], refs[group + 2 :]
    lanes, channels = own_ref.shape
    copies = [pltpu.make_async_copy(sources[k], buffer.at[k], sems.at[k]) for k in range(group)]
    for copy in copies:
        copy.start()
    inner = lax.rem(where_ref[0], group)
    level = where_ref[0] // group
    half = group // 2
    block = 512

    def partial(mask, cols, first):
        side = pl.ds(pl.multiple_of((level ^ mask) * lanes, lanes), lanes)
        total = None
        for k in range(first, first + half):
            part = rows_of(grads_ref[inner ^ k, :, side], buffer[k, :, cols])
            total = part if total is None else total + part
        return total

    for copy in copies[:half]:
        copy.wait()
    spans = [slice(start, start + block) for start in range(0, channels, block)]
    firsts = {(mask, n): partial(mask, cols, 0) for mask in (1, 0) for n, cols in enumerate(spans)}
    for copy in copies[half:]:
        copy.wait()
    for n, cols in enumerate(spans):
        send_ref[:, cols] = (firsts[1, n] + partial(1, cols, half)).astype(bf16)
        own_ref[:, cols] = firsts[0, n] + partial(0, cols, half)


def product_call(lanes, where, grads, mixers):
    group, rows, cut = grads.shape
    channels = mixers[0].shape[1]
    return pl.pallas_call(
        product_kernel,
        in_specs=[pl.BlockSpec(memory_space=pltpu.SMEM)]
        + held(1)
        + [pl.BlockSpec(memory_space=pl.ANY)] * group,
        out_specs=held(2),
        out_shape=[
            jax.ShapeDtypeStruct((lanes, channels), bf16),
            jax.ShapeDtypeStruct((lanes, channels), f32),
        ],
        scratch_shapes=[
            pltpu.VMEM((group, rows, channels), bf16),
            pltpu.SemaphoreType.DMA((group,)),
        ],
        compiler_params=params(24),
        cost_estimate=pl.CostEstimate(
            flops=2 * group * rows * cut * channels, bytes_accessed=6 << 20, transcendentals=0
        ),
        name="product",
    )(where, grads, *mixers)


def on_device(
    moe_input,
    cotangent,
    expert_ids,
    route_weight,
    gate_proj,
    up_proj,
    down_proj,
    out_weight,
    recur_input,
    gate_input,
    states,
    conv_taps,
    decay_gate_w,
    input_gate_w,
    decay_rate,
    decay_extra,
):
    experts = lax.axis_size("sp")
    cores = lax.axis_size("tp")
    place = lax.axis_index("sp")
    core = lax.axis_index("tp")
    group = 8 if experts % 8 == 0 else experts
    outer = experts // group
    tok_rows, width = moe_input.shape
    channels = recur_input.shape[1]
    top_count = expert_ids.shape[1]
    capacity = max(2, 4 * tok_rows // experts)
    share = capacity // cores
    own_slots = experts * share

    flat_ids = expert_ids.reshape(-1)
    onehot = (flat_ids[:, None] == jnp.arange(experts, dtype=jnp.int32)[None, :]).astype(jnp.int32)
    slot_rank = jnp.sum((jnp.cumsum(onehot, axis=0) - onehot) * onehot, axis=1)
    pair_slots = (flat_ids * capacity + slot_rank).reshape(tok_rows, top_count)
    slot_iota = jnp.arange(own_slots, dtype=jnp.int32)
    slot_ids = (slot_iota // share) * capacity + core * share + slot_iota % share
    hits = slot_ids[:, None, None] == pair_slots[None, :, :]
    placing = jnp.any(hits, axis=2).astype(bf16)
    send_rows = times(placing, moe_input).astype(bf16).reshape(experts, share, width)
    late = (gate_input, states, recur_input, cotangent, route_weight)
    send_rows, late = lax.optimization_barrier((send_rows, late))
    gate_input, states, recur_input, cotangent_late, route_weight = late
    got_rows = lax.all_to_all(send_rows, "sp", split_axis=0, concat_axis=0, tiled=True)
    own_weights = (gate_proj[0], up_proj[0], down_proj[0])
    other_weights = tuple(swapped(weight, "tp", 1) for weight in own_weights)
    edge = jnp.concatenate([recur_input[-3:].astype(f32), states[-1:]], axis=0)
    edge = shifted(edge, "sp", 1)
    slot_weight = jnp.sum(jnp.where(hits, route_weight[None, :, :], 0.0), axis=(1, 2))
    send_grads = times(placing, cotangent_late) * slot_weight[:, None]
    send_grads = send_grads.astype(bf16).reshape(experts, share, width)

    gate_float = gate_input.astype(f32)
    gelu_value, gelu_back = jax.vjp(jax.nn.gelu, gate_float)
    slope = states * gelu_back(jnp.ones_like(gate_float))[0]
    mixer_out = (states * gelu_value).astype(bf16)
    half = group // 2
    mixers = {0: mixer_out}
    mixers[half] = swapped(mixer_out, "sp", half)
    send_grads, gelu_value, slope, edge, got_rows = lax.optimization_barrier(
        (send_grads, gelu_value, slope, edge, got_rows)
    )
    got_grads = lax.all_to_all(send_grads, "sp", split_axis=0, concat_axis=0, tiled=True)
    for k in range(1, half):
        mixers[k] = swapped(mixer_out, "sp", k)
    extended = jnp.concatenate([edge[:3], recur_input.astype(f32)], axis=0)
    prev_state = edge[3:]
    taps = conv_taps.astype(f32)
    conv = taps[0] * extended[0:tok_rows]
    for tap in range(1, 4):
        conv = conv + taps[tap] * extended[tap : tap + tok_rows]
    blocks, block_width = decay_gate_w.shape[:2]
    conv_low = conv.astype(bf16)

    def by_block(value, weights):
        parts = [
            times(value[:, b * block_width : (b + 1) * block_width], weights[b]) for b in range(blocks)
        ]
        return jnp.concatenate(parts, axis=1)

    recur_gate = jax.nn.sigmoid(by_block(conv_low, decay_gate_w))
    input_gate = jax.nn.sigmoid(by_block(conv_low, input_gate_w))
    first_row = (place * tok_rows + jnp.arange(tok_rows, dtype=jnp.int32) == 0)[:, None]
    log_decay = -decay_scale * recur_gate * decay_rate[None, :] + decay_extra
    decay_value = jnp.exp(log_decay)
    mult = jnp.where(first_row, 1.0, jnp.sqrt(-jnp.expm1(2.0 * log_decay)))
    prev_states = jnp.concatenate([prev_state, states[:-1]], axis=0)
    next_decay = jnp.concatenate([decay_value[1:], jnp.ones((1, channels), f32)], axis=0)
    to_log = prev_states * decay_value - jnp.where(
        first_row, 0.0, input_gate * conv * decay_value * decay_value / mult
    )
    to_decay = to_log * (-decay_scale * decay_rate[None, :]) * recur_gate * (1.0 - recur_gate)
    to_input = mult * conv * input_gate * (1.0 - input_gate)
    direct = mult * input_gate

    rows_here = got_rows.reshape(own_slots, width)
    rows_there = swapped(rows_here, "tp", 1)
    rows_here, rows_there = lax.optimization_barrier((rows_here, rows_there))

    def first_half(gate_w, up_w):
        gate_pre = times(rows_here, gate_w)
        up_pre = times(rows_here, up_w)
        sigmoid_gate = jax.nn.sigmoid(gate_pre)
        silu_gate = gate_pre * sigmoid_gate
        slope_gate = up_pre * sigmoid_gate * (1.0 + gate_pre * (1.0 - sigmoid_gate))
        return (silu_gate * up_pre).astype(bf16), silu_gate.astype(bf16), slope_gate.astype(bf16)

    pres = tuple(first_half(weights[0], weights[1]) for weights in (own_weights, other_weights))
    head_coef = jnp.stack([to_decay[:8], to_input[:8], direct[:8]])
    gates = (
        next_decay, decay_value[:1], head_coef,
        to_decay.astype(bf16), to_input.astype(bf16), direct.astype(bf16),
    )
    got_grads, pres, gates = lax.optimization_barrier((got_grads, pres, gates))
    next_decay, first_decay, head_coef, to_decay, to_input, direct = gates
    for k in range(1, half):
        mixers[k ^ half] = swapped(mixers[half], "sp", k)
    grads_here = got_grads.reshape(own_slots, width)

    partial, gate_h, gate_o, up_h, up_o = expert_call(grads_here, pres, (own_weights, other_weights))
    own_grads, other_grads = (gate_h, up_h), (gate_o, up_o)
    shared = partial.reshape(experts, share, width)
    back = lax.all_to_all(shared, "sp", split_axis=0, concat_axis=0, tiled=True)
    head_coef = shifted(head_coef, "sp", -1)
    hidden_h, gate_h, up_h = pres[0][0], own_grads[0], own_grads[1]
    grads_there = swapped(grads_here, "tp", 1)
    hidden_t = swapped(pres[1][0], "tp", 1)
    gate_t = swapped(other_grads[0], "tp", 1)
    up_t = swapped(other_grads[1], "tp", 1)
    down_grad = rows_of(hidden_h, grads_here) + rows_of(hidden_t, grads_there)
    gate_weight_grad = rows_of(rows_here, gate_h) + rows_of(rows_there, gate_t)
    up_weight_grad = rows_of(rows_here, up_h) + rows_of(rows_there, up_t)
    weight_grads = (gate_weight_grad.astype(bf16), up_weight_grad.astype(bf16), down_grad.astype(bf16))
    back, weight_grads, head_coef, mixers = lax.optimization_barrier(
        (back, weight_grads, head_coef, mixers)
    )

    mine_back = rows_of(placing, back.reshape(own_slots, width)).astype(bf16)
    other_back = swapped(mine_back, "tp", 1)
    out_rows = width // experts
    where = place[None].astype(jnp.int32)
    input_grad, pieces = combine_call(mine_back, other_back, cotangent, group, out_rows)

    groups = [[base + peer for peer in range(group)] for base in range(0, experts, group)]
    grads = lax.all_to_all(
        pieces, "sp", split_axis=0, concat_axis=0, tiled=True, axis_index_groups=groups
    )
    gate_grad, local, cumul, ends, head = mixer_call(
        input_grad, out_weight, gelu_value, slope, next_decay, first_decay
    )
    head = shifted(head, "sp", -1)
    near = 4 if experts % 4 == 0 else experts
    ends = [ends] + [swapped(ends, "sp", k) for k in range(1, near)]
    grads, ends, head = lax.optimization_barrier((grads, ends, head))
    later, total = near_call(where, ends)
    later_next = shifted(later, "sp", -1)
    far = [total] + [swapped(total, "sp", k * near) for k in range(1, experts // near)]
    mixers = [mixers[k] for k in range(group)]
    received = []
    if outer == 2 and out_rows % 128 == 0:
        send, out_weight_grad = product_call(out_rows, where, grads, mixers)
        received.append(swapped(send, "sp", group))
    else:
        full = sum(
            rows_of(lax.dynamic_index_in_dim(grads, place % group ^ k, 0, False), mixers[k])
            for k in range(group)
        ).reshape(outer, out_rows, channels)

        def block_for(mask):
            return lax.dynamic_index_in_dim(full, place // group ^ mask, 0, False)

        for mask in range(1, outer):
            received.append(swapped(block_for(mask).astype(bf16), "sp", mask * group))
        out_weight_grad = block_for(0)
    for part in received:
        out_weight_grad = out_weight_grad + part.astype(f32)

    where = jnp.concatenate([where, jnp.full((1,), near, jnp.int32)])
    recur_grad = tail_call(
        where, later, later_next, far, local, cumul, to_decay, to_input, direct,
        head, head_coef, conv_taps, decay_gate_w, input_gate_w,
    )
    return (
        weight_grads[0][None],
        weight_grads[1][None],
        weight_grads[2][None],
        out_weight_grad,
        input_grad,
        recur_grad,
        gate_grad,
    )


def solution(mesh):
    return jax.shard_map(
        on_device,
        mesh=mesh,
        in_specs=(
            P("sp", None),
            P("sp", None),
            P("sp", None),
            P("sp", None),
            P("sp", None, "tp"),
            P("sp", None, "tp"),
            P("sp", "tp", None),
            P(None, "tp"),
            P("sp", "tp"),
            P("sp", "tp"),
            P("sp", "tp"),
            P(None, "tp"),
            P("tp", None, None),
            P("tp", None, None),
            P("tp"),
            P("sp", "tp"),
        ),
        out_specs=(
            P("sp", None, "tp"),
            P("sp", None, "tp"),
            P("sp", "tp", None),
            P("sp", "tp"),
            P("sp", None),
            P("sp", "tp"),
            P("sp", "tp"),
        ),
        check_vma=False,
    )
```

```python
import functools

import jax
import jax.numpy as jnp
from jax import lax
from jax.experimental import pallas as pl
from jax.experimental.pallas import tpu as pltpu
from jax.sharding import PartitionSpec as P


decay_scale = 8.0
f32 = jnp.float32
bf16 = jnp.bfloat16


def dot(left, right, contract):
    return lax.dot_general(left, right, (contract, ((), ())), preferred_element_type=f32)


def rows_of(left, right):
    return dot(left, right, ((0,), (0,)))


def cols_of(left, right):
    return dot(left, right, ((1,), (1,)))


def times(left, right):
    return dot(left, right, ((1,), (0,)))


def shifted(value, axis, steps):
    count = lax.axis_size(axis)
    pairs = [(s, s + steps) for s in range(max(0, -steps), min(count, count - steps))]
    return lax.ppermute(value, axis, pairs)


def swapped(value, axis, mask):
    count = lax.axis_size(axis)
    return lax.ppermute(value, axis, [(s, s ^ mask) for s in range(count)])


def back_scan(decays, values):
    rows = values.shape[0]
    inner = lax.broadcasted_iota(jnp.int32, values.shape, 0) % 8
    step = 1
    while step < rows:
        if step < 8:
            keep = inner < 8 - step
            later_a = jnp.where(keep, pltpu.roll(decays, rows - step, 0), 1.0)
            later_b = jnp.where(keep, pltpu.roll(values, rows - step, 0), 0.0)
            values = values + decays * later_b
            decays = decays * later_a
            step *= 2
        else:
            break
    tiles = rows // 8
    decay_out = [None] * tiles
    value_out = [None] * tiles
    carry_a = jnp.ones_like(values[:1])
    carry_b = jnp.zeros_like(values[:1])
    for tile in reversed(range(tiles)):
        part_a = decays[tile * 8 : tile * 8 + 8]
        part_b = values[tile * 8 : tile * 8 + 8]
        value_out[tile] = part_b + part_a * carry_b
        decay_out[tile] = part_a * carry_a
        carry_b = value_out[tile][:1]
        carry_a = decay_out[tile][:1]
    return decay_out, value_out


def held(count):
    return [pl.BlockSpec(memory_space=pltpu.VMEM)] * count


def params(mib):
    return pltpu.CompilerParams(vmem_limit_bytes=mib << 20)


def mixer_kernel(grad_ref, weight_ref, gelu_ref, slope_ref, next_ref, first_ref,
                 gate_ref, local_ref, cumul_ref, ends_ref, head_ref):
    mixer = jnp.dot(grad_ref[...], weight_ref[...], preferred_element_type=f32)
    gate_ref[...] = (mixer * slope_ref[...]).astype(bf16)
    decays, values = back_scan(next_ref[...], mixer * gelu_ref[...])
    for tile in range(0, len(values), 2):
        rows = slice(tile * 8, tile * 8 + 16)
        cumul_ref[rows] = jnp.concatenate(decays[tile : tile + 2], axis=0).astype(bf16)
        local_ref[rows] = jnp.concatenate(values[tile : tile + 2], axis=0).astype(bf16)
    head_ref[0] = values[0]
    head_ref[1] = decays[0]
    first = first_ref[...]
    both = jnp.concatenate([first * decays[0][:1], first * values[0][:1]], axis=0)
    for peer in range(ends_ref.shape[0]):
        ends_ref[peer] = both


def mixer_call(input_grad, out_weight, gelu, slope, next_decay, first, peers):
    rows, width = input_grad.shape
    channels = out_weight.shape[1]
    block = 256
    wide = pl.BlockSpec((rows, block), lambda i: (0, i))
    return pl.pallas_call(
        mixer_kernel,
        grid=(channels // block,),
        in_specs=[
            pl.BlockSpec((rows, width), lambda i: (0, 0)),
            pl.BlockSpec((width, block), lambda i: (0, i)),
            wide, wide, wide,
            pl.BlockSpec((1, block), lambda i: (0, i)),
        ],
        out_specs=[
            wide, wide, wide,
            pl.BlockSpec((peers, 2, block), lambda i: (0, 0, i)),
            pl.BlockSpec((2, 8, block), lambda i: (0, 0, i)),
        ],
        out_shape=[
            jax.ShapeDtypeStruct((rows, channels), bf16),
            jax.ShapeDtypeStruct((rows, channels), bf16),
            jax.ShapeDtypeStruct((rows, channels), bf16),
            jax.ShapeDtypeStruct((peers, 2, channels), f32),
            jax.ShapeDtypeStruct((2, 8, channels), f32),
        ],
        cost_estimate=pl.CostEstimate(
            flops=2 * rows * width * channels, bytes_accessed=8 << 20, transcendentals=0
        ),
        name="mixer",
    )(input_grad, out_weight, gelu, slope, next_decay, first)


def tail_kernel(where_ref, ends_ref, local_ref, cumul_ref, to_decay_ref, to_input_ref, direct_ref,
                head_ref, head_coef_ref, taps_ref, decay_w_ref, input_w_ref, out_ref):
    mine = where_ref[0]
    count = ends_ref.shape[0]
    block = decay_w_ref.shape[1]
    rows = local_ref.shape[0]
    taps = taps_ref[...].astype(f32)

    carry = jnp.zeros_like(local_ref[:1])
    head_carry = carry
    for place in reversed(range(1, count)):
        ends = ends_ref[place]
        longer = ends[1:2] + ends[0:1] * carry
        head_carry = jnp.where(place > mine + 1, longer, head_carry)
        carry = jnp.where(place > mine, longer, carry)

    for index in range(decay_w_ref.shape[0]):
        cols = slice(index * block, (index + 1) * block)
        decay_w = decay_w_ref[index]

        def wide(ref):
            return ref[:, cols].astype(f32)

        input_w = input_w_ref[index]

        def conv_grad(carried, to_decay, to_input, direct):
            decay_pre = (carried * to_decay).astype(bf16)
            input_pre = (carried * to_input).astype(bf16)
            return carried * direct + cols_of(decay_pre, decay_w) + cols_of(input_pre, input_w)

        main = conv_grad(
            wide(local_ref) + wide(cumul_ref) * carry[:, cols],
            wide(to_decay_ref), wide(to_input_ref), wide(direct_ref),
        )
        halo = conv_grad(
            head_ref[0, :, cols] + head_ref[1, :, cols] * head_carry[:, cols],
            head_coef_ref[0, :, cols], head_coef_ref[1, :, cols], head_coef_ref[2, :, cols],
        )
        whole = jnp.concatenate([main, halo], axis=0)
        total = taps[0:1, cols] * pltpu.roll(whole, whole.shape[0] - 3, 0)
        for tap in range(1, 3):
            total = total + taps[tap : tap + 1, cols] * pltpu.roll(whole, whole.shape[0] - 3 + tap, 0)
        total = total + taps[3:4, cols] * whole
        out_ref[:, cols] = total[:rows].astype(bf16)


def tail_call(where, *arrays):
    ends, local, decay_w = arrays[0], arrays[1], arrays[-1]
    rows, channels = local.shape
    width = decay_w.shape[1]
    block = 2 * width
    wide = pl.BlockSpec((rows, block), lambda i, s: (0, i))
    gate = pl.BlockSpec((2, width, width), lambda i, s: (i, 0, 0))
    return pl.pallas_call(
        tail_kernel,
        grid_spec=pltpu.PrefetchScalarGridSpec(
            num_scalar_prefetch=1,
            grid=(channels // block,),
            in_specs=[
                pl.BlockSpec((ends.shape[0], 2, block), lambda i, s: (0, 0, i)),
                wide, wide, wide, wide, wide,
                pl.BlockSpec((2, 8, block), lambda i, s: (0, 0, i)),
                pl.BlockSpec((3, 8, block), lambda i, s: (0, 0, i)),
                pl.BlockSpec((4, block), lambda i, s: (0, i)),
                gate, gate,
            ],
            out_specs=wide,
        ),
        out_shape=jax.ShapeDtypeStruct((rows, channels), bf16),
        cost_estimate=pl.CostEstimate(
            flops=8 * rows * width * channels, bytes_accessed=7 << 20, transcendentals=0
        ),
        name="tail",
    )(where, *arrays)


def combine_kernel(lanes, mine_ref, other_ref, cot_ref, grad_ref, piece_ref):
    group, _, cut = piece_ref.shape
    for peer in range(group):
        for level in range(cut // lanes):
            column = (level * group + peer) * lanes
            cols = slice(column, column + lanes)
            total = mine_ref[:, cols].astype(f32) + other_ref[:, cols].astype(f32)
            total = (total + cot_ref[:, cols].astype(f32)).astype(bf16)
            grad_ref[:, cols] = total
            piece_ref[peer, :, level * lanes : (level + 1) * lanes] = total


def combine_call(mine, other, cotangent, group, lanes):
    rows, width = mine.shape
    return pl.pallas_call(
        functools.partial(combine_kernel, lanes),
        in_specs=held(3),
        out_specs=held(2),
        out_shape=[
            jax.ShapeDtypeStruct((rows, width), bf16),
            jax.ShapeDtypeStruct((group, rows, width // group), bf16),
        ],
        compiler_params=params(10),
        cost_estimate=pl.CostEstimate(flops=1 << 28, bytes_accessed=5 << 20, transcendentals=0),
        name="combine",
    )(mine, other, cotangent)


def product_kernel(where_ref, grads_ref, *refs):
    group, _, _ = grads_ref.shape
    sources, (send_ref, own_ref), (buffer, sems) = refs[:group], refs[group : group + 2], refs[group + 2 :]
    lanes, channels = own_ref.shape
    copies = [pltpu.make_async_copy(sources[k], buffer.at[k], sems.at[k]) for k in range(group)]
    for copy in copies:
        copy.start()
    inner = lax.rem(where_ref[0], group)
    level = where_ref[0] // group
    half = group // 2
    block = 512

    def partial(mask, cols, first):
        side = pl.ds(pl.multiple_of((level ^ mask) * lanes, lanes), lanes)
        total = None
        for k in range(first, first + half):
            part = rows_of(grads_ref[inner ^ k, :, side], buffer[k, :, cols])
            total = part if total is None else total + part
        return total

    for copy in copies[:half]:
        copy.wait()
    spans = [slice(start, start + block) for start in range(0, channels, block)]
    firsts = {(mask, n): partial(mask, cols, 0) for mask in (1, 0) for n, cols in enumerate(spans)}
    for copy in copies[half:]:
        copy.wait()
    for n, cols in enumerate(spans):
        send_ref[:, cols] = (firsts[1, n] + partial(1, cols, half)).astype(bf16)
        own_ref[:, cols] = firsts[0, n] + partial(0, cols, half)


def product_call(lanes, where, grads, mixers):
    group, rows, cut = grads.shape
    channels = mixers[0].shape[1]
    return pl.pallas_call(
        product_kernel,
        in_specs=[pl.BlockSpec(memory_space=pltpu.SMEM)]
        + held(1)
        + [pl.BlockSpec(memory_space=pl.ANY)] * group,
        out_specs=held(2),
        out_shape=[
            jax.ShapeDtypeStruct((lanes, channels), bf16),
            jax.ShapeDtypeStruct((lanes, channels), f32),
        ],
        scratch_shapes=[
            pltpu.VMEM((group, rows, channels), bf16),
            pltpu.SemaphoreType.DMA((group,)),
        ],
        compiler_params=params(24),
        cost_estimate=pl.CostEstimate(
            flops=2 * group * rows * cut * channels, bytes_accessed=6 << 20, transcendentals=0
        ),
        name="product",
    )(where, grads, *mixers)


def on_device(
    moe_input,
    cotangent,
    expert_ids,
    route_weight,
    gate_proj,
    up_proj,
    down_proj,
    out_weight,
    recur_input,
    gate_input,
    states,
    conv_taps,
    decay_gate_w,
    input_gate_w,
    decay_rate,
    decay_extra,
):
    experts = lax.axis_size("sp")
    cores = lax.axis_size("tp")
    place = lax.axis_index("sp")
    core = lax.axis_index("tp")
    group = 8 if experts % 8 == 0 else experts
    outer = experts // group
    tok_rows, width = moe_input.shape
    channels = recur_input.shape[1]
    top_count = expert_ids.shape[1]
    capacity = max(2, 4 * tok_rows // experts)
    share = capacity // cores
    own_slots = experts * share

    flat_ids = expert_ids.reshape(-1)
    onehot = (flat_ids[:, None] == jnp.arange(experts, dtype=jnp.int32)[None, :]).astype(jnp.int32)
    slot_rank = jnp.sum((jnp.cumsum(onehot, axis=0) - onehot) * onehot, axis=1)
    pair_slots = (flat_ids * capacity + slot_rank).reshape(tok_rows, top_count)
    slot_iota = jnp.arange(own_slots, dtype=jnp.int32)
    slot_ids = (slot_iota // share) * capacity + core * share + slot_iota % share
    hits = slot_ids[:, None, None] == pair_slots[None, :, :]
    placing = jnp.any(hits, axis=2).astype(bf16)
    send_rows = times(placing, moe_input).astype(bf16).reshape(experts, share, width)
    late = (gate_input, states, recur_input, cotangent, route_weight)
    send_rows, late = lax.optimization_barrier((send_rows, late))
    gate_input, states, recur_input, cotangent_late, route_weight = late
    got_rows = lax.all_to_all(send_rows, "sp", split_axis=0, concat_axis=0, tiled=True)
    own_weights = (gate_proj[0], up_proj[0], down_proj[0])
    other_weights = tuple(swapped(weight, "tp", 1) for weight in own_weights)
    edge = jnp.concatenate([recur_input[-3:].astype(f32), states[-1:]], axis=0)
    edge = shifted(edge, "sp", 1)
    slot_weight = jnp.sum(jnp.where(hits, route_weight[None, :, :], 0.0), axis=(1, 2))
    send_grads = times(placing, cotangent_late) * slot_weight[:, None]
    send_grads = send_grads.astype(bf16).reshape(experts, share, width)

    gate_float = gate_input.astype(f32)
    gelu_value, gelu_back = jax.vjp(jax.nn.gelu, gate_float)
    slope = states * gelu_back(jnp.ones_like(gate_float))[0]
    mixer_out = (states * gelu_value).astype(bf16)
    half = group // 2
    mixers = {0: mixer_out}
    mixers[half] = swapped(mixer_out, "sp", half)
    weights = tuple(
        jnp.concatenate([own, other], axis=axis)
        for own, other, axis in zip(own_weights, other_weights, (1, 1, 0))
    )
    send_grads, gelu_value, slope, edge, got_rows, weights = lax.optimization_barrier(
        (send_grads, gelu_value, slope, edge, got_rows, weights)
    )
    got_grads = lax.all_to_all(send_grads, "sp", split_axis=0, concat_axis=0, tiled=True)
    for k in range(1, half):
        mixers[k] = swapped(mixer_out, "sp", k)
    extended = jnp.concatenate([edge[:3], recur_input.astype(f32)], axis=0)
    prev_state = edge[3:]
    taps = conv_taps.astype(f32)
    conv = taps[0] * extended[0:tok_rows]
    for tap in range(1, 4):
        conv = conv + taps[tap] * extended[tap : tap + tok_rows]
    blocks, block_width = decay_gate_w.shape[:2]
    conv_low = conv.astype(bf16)

    def by_block(value, weights):
        parts = [
            times(value[:, b * block_width : (b + 1) * block_width], weights[b]) for b in range(blocks)
        ]
        return jnp.concatenate(parts, axis=1)

    recur_gate = jax.nn.sigmoid(by_block(conv_low, decay_gate_w))
    input_gate = jax.nn.sigmoid(by_block(conv_low, input_gate_w))
    first_row = (place * tok_rows + jnp.arange(tok_rows, dtype=jnp.int32) == 0)[:, None]
    log_decay = -decay_scale * recur_gate * decay_rate[None, :] + decay_extra
    decay_value = jnp.exp(log_decay)
    mult = jnp.where(first_row, 1.0, jnp.sqrt(-jnp.expm1(2.0 * log_decay)))
    prev_states = jnp.concatenate([prev_state, states[:-1]], axis=0)
    next_decay = jnp.concatenate([decay_value[1:], jnp.ones((1, channels), f32)], axis=0)
    to_log = prev_states * decay_value - jnp.where(
        first_row, 0.0, input_gate * conv * decay_value * decay_value / mult
    )
    to_decay = to_log * (-decay_scale * decay_rate[None, :]) * recur_gate * (1.0 - recur_gate)
    to_input = mult * conv * input_gate * (1.0 - input_gate)
    direct = mult * input_gate

    rows_here = got_rows.reshape(own_slots, width)
    rows_there = swapped(rows_here, "tp", 1)
    rows_here, rows_there = lax.optimization_barrier((rows_here, rows_there))

    def first_half(gate_w, up_w):
        gate_pre = times(rows_here, gate_w)
        up_pre = times(rows_here, up_w)
        sigmoid_gate = jax.nn.sigmoid(gate_pre)
        silu_gate = gate_pre * sigmoid_gate
        slope_gate = up_pre * sigmoid_gate * (1.0 + gate_pre * (1.0 - sigmoid_gate))
        return (silu_gate * up_pre).astype(bf16), silu_gate.astype(bf16), slope_gate.astype(bf16)

    pres = first_half(weights[0], weights[1])
    head_coef = jnp.stack([to_decay[:8], to_input[:8], direct[:8]])
    gates = (
        next_decay, decay_value[:1], head_coef,
        to_decay.astype(bf16), to_input.astype(bf16), direct.astype(bf16),
    )
    got_grads, pres, gates = lax.optimization_barrier((got_grads, pres, gates))
    next_decay, first_decay, head_coef, to_decay, to_input, direct = gates
    for k in range(1, half):
        mixers[k ^ half] = swapped(mixers[half], "sp", k)
    grads_here = got_grads.reshape(own_slots, width)

    def second_half(pre, down_w):
        hidden_grad = cols_of(grads_here, down_w)
        return (hidden_grad * pre[2].astype(f32)).astype(bf16), (hidden_grad * pre[1].astype(f32)).astype(bf16)

    gate_grads, up_grads = second_half(pres, weights[2])
    partial = cols_of(gate_grads, weights[0]) + cols_of(up_grads, weights[1])
    shared = partial.astype(bf16).reshape(experts, share, width)
    back = lax.all_to_all(shared, "sp", split_axis=0, concat_axis=0, tiled=True)
    head_coef = shifted(head_coef, "sp", -1)
    units = own_weights[0].shape[1]
    (hidden_h, hidden_o), (gate_h, gate_o), (up_h, up_o) = (
        (value[:, :units], value[:, units:]) for value in (pres[0], gate_grads, up_grads)
    )
    grads_there = swapped(grads_here, "tp", 1)
    hidden_t = swapped(hidden_o, "tp", 1)
    gate_t = swapped(gate_o, "tp", 1)
    up_t = swapped(up_o, "tp", 1)
    down_grad = rows_of(hidden_h, grads_here) + rows_of(hidden_t, grads_there)
    gate_weight_grad = rows_of(rows_here, gate_h) + rows_of(rows_there, gate_t)
    up_weight_grad = rows_of(rows_here, up_h) + rows_of(rows_there, up_t)
    weight_grads = (gate_weight_grad.astype(bf16), up_weight_grad.astype(bf16), down_grad.astype(bf16))
    back, weight_grads, head_coef, mixers = lax.optimization_barrier(
        (back, weight_grads, head_coef, mixers)
    )

    mine_back = rows_of(placing, back.reshape(own_slots, width)).astype(bf16)
    other_back = swapped(mine_back, "tp", 1)
    out_rows = width // experts
    where = place[None].astype(jnp.int32)
    input_grad, pieces = combine_call(mine_back, other_back, cotangent, group, out_rows)

    groups = [[base + peer for peer in range(group)] for base in range(0, experts, group)]
    grads = lax.all_to_all(
        pieces, "sp", split_axis=0, concat_axis=0, tiled=True, axis_index_groups=groups
    )
    gate_grad, local, cumul, ends, head = mixer_call(
        input_grad, out_weight, gelu_value, slope, next_decay, first_decay, experts
    )
    head = shifted(head, "sp", -1)
    ends = lax.all_to_all(ends, "sp", split_axis=0, concat_axis=0, tiled=True)
    mixers = [mixers[k] for k in range(group)]
    received = []
    if outer == 2 and out_rows % 128 == 0:
        send, out_weight_grad = product_call(out_rows, where, grads, mixers)
        received.append(swapped(send, "sp", group))
    else:
        full = sum(
            rows_of(lax.dynamic_index_in_dim(grads, place % group ^ k, 0, False), mixers[k])
            for k in range(group)
        ).reshape(outer, out_rows, channels)

        def block_for(mask):
            return lax.dynamic_index_in_dim(full, place // group ^ mask, 0, False)

        for mask in range(1, outer):
            received.append(swapped(block_for(mask).astype(bf16), "sp", mask * group))
        out_weight_grad = block_for(0)
    for part in received:
        out_weight_grad = out_weight_grad + part.astype(f32)

    recur_grad = tail_call(
        where, ends, local, cumul, to_decay, to_input, direct,
        head, head_coef, conv_taps, decay_gate_w, input_gate_w,
    )
    return (
        weight_grads[0][None],
        weight_grads[1][None],
        weight_grads[2][None],
        out_weight_grad,
        input_grad,
        recur_grad,
        gate_grad,
    )


def solution(mesh):
    return jax.shard_map(
        on_device,
        mesh=mesh,
        in_specs=(
            P("sp", None),
            P("sp", None),
            P("sp", None),
            P("sp", None),
            P("sp", None, "tp"),
            P("sp", None, "tp"),
            P("sp", "tp", None),
            P(None, "tp"),
            P("sp", "tp"),
            P("sp", "tp"),
            P("sp", "tp"),
            P(None, "tp"),
            P("tp", None, None),
            P("tp", None, None),
            P("tp"),
            P("sp", "tp"),
        ),
        out_specs=(
            P("sp", None, "tp"),
            P("sp", None, "tp"),
            P("sp", "tp", None),
            P("sp", "tp"),
            P("sp", None),
            P("sp", "tp"),
            P("sp", "tp"),
        ),
        check_vma=False,
    )
```
